256 devices in a mesh: sp: 64 (over z, y, core), tp: 4 (over x).
Axes of the slice: x: 4, y: 4, z: 8, core: 2. Of those that a mesh axis runs over, the one named last changes fastest.
Arguments:
- tokens: bfloat16 [4, 24576, 2048], P(None, 'sp'), may hold values from -21 to 21
- query_weight: bfloat16 [2048, 1024], P(None, 'tp'), may hold values from -0.125 to 0.125
- key_weight: bfloat16 [2048, 1024], P(None, 'tp'), may hold values from -0.125 to 0.125
- value_weight: bfloat16 [2048, 1024], P(None, 'tp'), may hold values from -0.125 to 0.125
- out_gain: float32 [1024], replicated, may hold values from 0.1 to 1.9
- out_weight: bfloat16 [1024, 2048], P(None, 'tp'), may hold values from -0.1875 to 0.1875
Outputs:
- mixed_out: bfloat16 [4, 24576, 2048], P(None, 'sp', 'tp')
- total_log: float32 [4, 8, 24576], P(None, 'tp', 'sp')
The draws below stay inside these ranges and needn't reach their ends.
All inputs are finite; a program needn't handle non-finite values.
Results may differ from the reference program's by a relative error of at most 0.0098.
Values may be sent and summed in bfloat16 or wider, within the bound.
A program may use at most 128 MiB of HBM per device.

```python
import jax
import jax.numpy as jnp
from jax import lax

D = 2048
HEADS = 8
HEAD_DIM = 128
REACH = 64
SEQS = 4
TOK_DEV = 384
TOKENS = 24576


def draw_tokens(key, part):
    dims = (SEQS, TOKENS, D)
    return jnp.clip(jax.random.normal(key, dims, jnp.float32), -6.0, 6.0).astype(jnp.bfloat16)


def block_levels(rng, shape, cuts, least, high):
    factor_of, own = 1.0, jax.random.fold_in(rng, 6)
    for axis_at, blocks in cuts:
        heights = jnp.exp(jax.random.uniform(jax.random.fold_in(own, axis_at), (blocks,), jnp.float32, least / len(cuts), high / len(cuts)))
        factor_of = factor_of * jnp.repeat(heights, shape[axis_at] // blocks).reshape([-1 if axis == axis_at else 1 for axis in range(len(shape))])
    return factor_of


def bell_draw(rng, shape, deviation, bound, cuts=(), kind=jnp.bfloat16):
    entries = jax.random.normal(rng, shape, jnp.float32) * deviation
    if len(cuts) > 0:
        entries = block_levels(rng, shape, cuts, -0.22, 0.18) * entries
    return jnp.clip(entries, min=-bound, max=bound).astype(kind)


def setup_inputs(seed: int = 0) -> dict:
    arg_keys = jax.random.split(jax.random.key(seed), 7)
    tokens = draw_tokens(jax.random.fold_in(arg_keys[6], 71), 0)
    query_weight = bell_draw(arg_keys[1], (D, HEADS * HEAD_DIM), D ** -0.5, 0.125, ((1, 4),))
    key_weight = bell_draw(arg_keys[2], (D, HEADS * HEAD_DIM), D ** -0.5, 0.125, ((1, 4),))
    value_weight = bell_draw(arg_keys[3], (D, HEADS * HEAD_DIM), D ** -0.5, 0.125, ((1, 4),))
    out_gain = jnp.clip(1.0 + 0.18 * jax.random.normal(arg_keys[4], (HEADS * HEAD_DIM,), jnp.float32), 0.1, 1.9)
    out_weight = bell_draw(arg_keys[5], (HEADS * HEAD_DIM, D), (HEADS * HEAD_DIM) ** -0.5, 0.1875, ((1, 4),))
    return {"tokens": tokens, "query_weight": query_weight, "key_weight": key_weight, "value_weight": value_weight, "out_gain": out_gain, "out_weight": out_weight}


DILATIONS = (1, 4, 16)
ROPE_BASE = 10000.0
MASK_FILL = -1e+30
NORM_FLOOR = 1e-06

def rotate(projected, positions):
    in_shape = projected.shape
    heads_view = projected.reshape(in_shape[0], in_shape[1], -1, HEAD_DIM)
    half_dim = HEAD_DIM // 2
    frequency = ROPE_BASE ** (-jnp.arange(half_dim, dtype=jnp.float32) / half_dim)
    angles = positions.astype(jnp.float32)[:, None] * frequency[None, :]
    cosine = jnp.cos(angles)[None, :, None, :]
    sine_part = jnp.sin(angles)[None, :, None, :]
    lower_half = heads_view[..., :half_dim]
    upper_half = heads_view[..., half_dim:]
    turned = jnp.concatenate([lower_half * cosine - upper_half * sine_part, upper_half * cosine + lower_half * sine_part], axis=-1)
    return turned.reshape(in_shape)

def band_attend(queries, extended, dilation, offset, total_len):
    seq_count, length, channels = queries.shape
    head_count = channels // HEAD_DIM
    reach_span = REACH * dilation
    query_rows = length // dilation
    key_rows = query_rows + 2 * REACH
    shaped_q = queries.reshape(seq_count, query_rows, dilation, head_count, HEAD_DIM).astype(jnp.float32)
    shaped_k = extended[:, :, :channels].reshape(seq_count, key_rows, dilation, head_count, HEAD_DIM).astype(jnp.float32)
    shaped_v = extended[:, :, channels:].reshape(seq_count, key_rows, dilation, head_count, HEAD_DIM).astype(jnp.float32)
    scores = jnp.einsum('sarhe,sbrhe->srhab', shaped_q, shaped_k)
    query_row = jnp.arange(query_rows, dtype=jnp.int32)[:, None]
    key_row = jnp.arange(key_rows, dtype=jnp.int32)[None, :]
    inband = (key_row >= query_row) & (key_row <= query_row + 2 * REACH)
    residue = jnp.arange(dilation, dtype=jnp.int32)[:, None, None]
    key_pos = offset - reach_span + key_row[None] * dilation + residue
    allowed = inband[None] & (key_pos >= 0) & (key_pos < total_len)
    scores = jnp.where(allowed[None, :, None], scores * HEAD_DIM ** (-0.5), MASK_FILL)
    maximum = lax.optimization_barrier(jnp.max(scores, axis=-1, keepdims=True))
    exp_scores = jnp.exp(scores - maximum)
    weight_sum = lax.optimization_barrier(jnp.sum(exp_scores, axis=-1, keepdims=True))
    probs = lax.optimization_barrier(exp_scores.astype(jnp.bfloat16)).astype(jnp.float32)
    branch = jnp.einsum('srhab,sbrhe->sarhe', probs, shaped_v)
    branch = branch / jnp.transpose(weight_sum, (0, 3, 1, 2, 4))
    branch = branch.reshape(seq_count, length, head_count, HEAD_DIM)
    log_sum = (maximum + jnp.log(weight_sum))[..., 0]
    log_sum = jnp.transpose(log_sum, (0, 2, 3, 1)).reshape(seq_count, head_count, length)
    return (branch, log_sum)

def combine(branch_out, branch_log):
    logs = jnp.stack(branch_log, 0)
    peak = lax.optimization_barrier(jnp.max(logs, axis=0))
    total_log = peak + jnp.log(lax.optimization_barrier(jnp.sum(jnp.exp(logs - peak[None]), axis=0)))
    shares = jnp.exp(logs - total_log[None])
    shares = jnp.transpose(shares, (0, 1, 3, 2))[..., None]
    merged = lax.optimization_barrier(jnp.sum(shares * jnp.stack(branch_out, 0), axis=0))
    seq_count, length, head_count, head_dim = merged.shape
    return (merged.reshape(seq_count, length, head_count * head_dim).astype(jnp.bfloat16), total_log)

def reference(tokens, query_weight, key_weight, value_weight, out_gain, out_weight):
    flat_rows = tokens.reshape(SEQS * TOKENS, D)
    positions = jnp.arange(TOKENS, dtype=jnp.int32)

    def project(weight):
        return jnp.dot(flat_rows, weight, preferred_element_type=jnp.float32).reshape(SEQS, TOKENS, -1)
    queries = rotate(project(query_weight), positions).astype(jnp.bfloat16)
    key_rows = rotate(project(key_weight), positions).astype(jnp.bfloat16)
    values = project(value_weight).astype(jnp.bfloat16)
    wide_span = REACH * DILATIONS[2]
    stacked = jnp.pad(jnp.concatenate([key_rows, values], axis=2), ((0, 0), (wide_span, wide_span), (0, 0)))

    def one_block(block_index):
        row_start = (block_index * TOK_DEV).astype(jnp.int32)
        block_q = lax.dynamic_slice_in_dim(queries, row_start, TOK_DEV, 1)
        branch_out = []
        branch_log = []
        for dilation in DILATIONS:
            reach_span = REACH * dilation
            extended = lax.dynamic_slice_in_dim(stacked, row_start + wide_span - reach_span, TOK_DEV + 2 * reach_span, 1)
            branch, log_sum = band_attend(block_q, extended, dilation, row_start, TOKENS)
            branch_out.append(branch)
            branch_log.append(log_sum)
        return combine(branch_out, branch_log)
    merged, total_log = lax.map(one_block, jnp.arange(TOKENS // TOK_DEV, dtype=jnp.int32))
    merged = jnp.transpose(merged, (1, 0, 2, 3)).reshape(SEQS, TOKENS, HEADS * HEAD_DIM)
    total_log = jnp.transpose(total_log, (1, 2, 0, 3)).reshape(SEQS, HEADS, TOKENS)
    lifted = merged.astype(jnp.float32)
    square = lax.optimization_barrier(jnp.mean(lifted * lifted, axis=-1))
    scaled = (lifted * out_gain.astype(jnp.float32)).astype(jnp.bfloat16)
    projected = jnp.dot(scaled.reshape(SEQS * TOKENS, HEADS * HEAD_DIM), out_weight, preferred_element_type=jnp.float32).reshape(SEQS, TOKENS, D)
    mixed_out = (projected * lax.rsqrt(square + NORM_FLOOR)[..., None]).astype(jnp.bfloat16)
    return (mixed_out, total_log)
```

```python
import functools
import math

import jax
import jax.numpy as jnp
import numpy as np
from jax import lax
from jax.experimental import pallas as pl
from jax.experimental.pallas import tpu as pltpu
from jax.sharding import PartitionSpec as P

HEAD_DIM = 128
REACH = 64
FAR = 16
NEAR = 4
GRAN = FAR * FAR
ROPE_BASE = 10000.0
MASK_FILL = -1e30
NORM_FLOOR = 1e-06
LOG2E = 1.0 / math.log(2.0)
LN2 = math.log(2.0)
F32 = jnp.float32
BF16 = jnp.bfloat16

MESH = pl.DeviceIdType.MESH


def iota(shape, dim):
    return lax.broadcasted_iota(jnp.int32, shape, dim)


def perm_token(p):
    slot = p // FAR
    a = p % FAR
    residue = slot // NEAR + NEAR * (slot % (FAR // NEAR))
    return a * FAR + residue


def dot_t(a, b):
    return lax.dot_general(a, b, (((1,), (1,)), ((), ())), preferred_element_type=F32)


def layer_kernel(
    nsp, tok_h, wq_h, wk_h, wv_h, wo_h, cos_h, sin_h, cos_base, sin_base, gain,
    out, log_out,
    tok, wq, wk, wv, wo, cos, sin, kn, qn, kvs, qs, gath, outs, logs, lsend, lrow,
    kp, qp, mp, on, perm, bias1, bias4, bias16, o1, m1, l1,
    load_sem, send_sem, recv_sem,
):
    half = tok.shape[0] // 2
    units = kn.shape[0]
    length = tok.shape[1]
    block = 2 * length
    grans = block // GRAN
    wide = REACH * FAR
    side = wide // GRAN
    tail = wide - block
    span = block + 2 * wide
    rows = block // FAR
    key_rows = span // FAR
    near_rows = rows + 2 * FAR
    cols = wq.shape[1]
    heads = cols // HEAD_DIM
    total = nsp * length
    scale = HEAD_DIM**-0.5 * LOG2E
    sp, t = lax.axis_index("sp"), lax.axis_index("tp")
    y, blk = sp % 2, sp // 2
    twin = sp + 1 - 2 * y
    right, left, opposite = (t + 1) % 4, (t + 3) % 4, (t + 2) % 4
    mine, other = y * half, (1 - y) * half

    loads = []

    def load(src, dst):
        copy = pltpu.make_async_copy(src, dst, load_sem.at[len(loads)])
        copy.start()
        loads.append(copy)
        return copy

    got_cos, got_sin = load(cos_h, cos), load(sin_h, sin)
    got_wk, got_wv = load(wk_h, wk), load(wv_h, wv)
    got_tok = {("m", 0): load(tok_h.at[mine], tok.at[0])}

    barrier = pltpu.get_barrier_semaphore()
    has = {d: (sp + d >= 0) & (sp + d < nsp) for d in (2, -2, 4, -4)}
    reach = {d: has[d] & has[-d] for d in (2, -2)}
    for peer in ((twin, t), (sp, right), (sp, left)):
        pl.semaphore_signal(barrier, inc=1, device_id=peer, device_id_type=MESH)
    count = 3
    for d in (2, -2):
        there = has[d]
        count = count + there.astype(jnp.int32)

        @pl.when(there)
        def _(d=d):
            pl.semaphore_signal(barrier, inc=1, device_id=(sp + d, t), device_id_type=MESH)

    first = pl.multiple_of(y * length, HEAD_DIM)
    second = pl.multiple_of((1 - y) * length, HEAD_DIM)

    def clear(d, at, size):
        @pl.when(jnp.logical_not(has[d]))
        def _():
            for u in range(units):
                kn[u, at : at + size] = jnp.zeros((size, kn.shape[2]), BF16)

    clear(-4, 0, tail)
    clear(-2, tail, block)
    clear(2, wide + block, block)
    clear(4, span - tail, tail)

    numbers = {}

    def copy(name, src, dst, peer):
        n = numbers.setdefault(name, len(numbers))
        return pltpu.make_async_remote_copy(
            src_ref=src, dst_ref=dst, send_sem=send_sem.at[n], recv_sem=recv_sem.at[n],
            device_id=peer, device_id_type=MESH,
        )

    sent = []

    def start(c):
        c.start()
        sent.append((c, None))

    def z_copy(kind, u, d):
        if kind == "T":
            src = wide - tail if d > 0 else wide + block
            dst = 0 if d > 0 else span - tail
            size = tail
        else:
            part = first if kind == "A" else second
            src = wide + part
            dst = (tail if d > 0 else wide + block) + part
            size = length
        return copy(
            (kind, u, d), kn.at[u, pl.ds(src, size)], kn.at[u, pl.ds(dst, size)], (sp + d, t)
        )

    def z_start(kind, u):
        for d in (2, -2):
            c = z_copy(kind, u, d)
            there = reach[d] if kind == "T" else has[d]

            @pl.when(there)
            def _():
                c.start()

            sent.append((c, there))

    def z_wait(kind, u):
        for d in (2, -2):

            @pl.when(has[-2 * d] if kind == "T" else has[-d])
            def _():
                z_copy(kind, u, d).wait_recv()

    def turned(x, w, store):
        a = jnp.dot(x, w[...], preferred_element_type=F32)
        for h in range(heads):
            one = a[:, h * HEAD_DIM : (h + 1) * HEAD_DIM]
            store(h, (one * cos[...] + pltpu.roll(one, HEAD_DIM // 2, 1) * sin[...]).astype(BF16))

    def lanes(n):
        return slice(n * HEAD_DIM, (n + 1) * HEAD_DIM)

    def keys_values(x, put):
        turned(x, wk, lambda h, a: put(2 * h, a))
        v = jnp.dot(x, wv[...], preferred_element_type=F32).astype(BF16)
        for h in range(heads):
            put(2 * h + 1, v[:, lanes(h)])

    def own_kv(s):
        def put(n, a):
            kn[s * heads + n // 2, pl.ds(wide + first, length), lanes(n % 2)] = a

        keys_values(tok[2 * s], put)

    def twin_kv(s):
        def put(n, a):
            kvs[s * heads + n // 2, :, lanes(n % 2)] = a

        keys_values(tok[2 * s + 1], put)

    def own_q(s):
        def put(n, a):
            qn[s * heads + n, pl.ds(first, length)] = a

        turned(tok[2 * s], wq, put)

    def twin_q(s):
        def put(n, a):
            qs[s * heads + n] = a

        turned(tok[2 * s + 1], wq, put)

    def y_kv(u, at):
        return copy(("yk", u), kvs.at[u], kn.at[u, pl.ds(wide + at, length)], (twin, t))

    def y_q(u, at):
        return copy(("yq", u), qs.at[u], qn.at[u, pl.ds(at, length)], (twin, t))

    def of(s):
        return range(s * heads, (s + 1) * heads)

    cos_at, sin_at = cos_base[pl.ds(sp, 1)], sin_base[pl.ds(sp, 1)]
    sign = jnp.where(iota(cos.shape, 1) < HEAD_DIM // 2, -1.0, 1.0)
    got_cos.wait()
    got_sin.wait()
    cos_step, sin_step = cos[...], sin[...]
    cos[...] = cos_step * cos_at - sin_step * sin_at
    sin[...] = (sin_step * cos_at + cos_step * sin_at) * sign
    for c in (got_wk, got_wv, got_tok["m", 0]):
        c.wait()
    got_tok["o", 0] = load(tok_h.at[other], tok.at[1])
    own_kv(0)
    pl.semaphore_wait(barrier, count)
    for u in of(0):
        z_start("A", u)
    got_tok["o", 0].wait()
    got_wq = load(wq_h, wq)
    for s in range(1, half):
        got_tok["o", s] = load(tok_h.at[other + s], tok.at[2 * s + 1])
        got_tok["m", s] = load(tok_h.at[mine + s], tok.at[2 * s])
    got_wo = load(wo_h, wo)
    twin_kv(0)
    for u in of(0):
        start(y_kv(u, first))
    got_wq.wait()
    twin_q(0)
    for u in of(0):
        start(y_q(u, first))
    for s in range(1, half):
        got_tok["o", s].wait()
        got_tok["m", s].wait()
        twin_kv(s)
        for u in of(s):
            start(y_kv(u, first))
        own_kv(s)
    y_kv(0, second).wait_recv()
    z_start("B", 0)
    own_q(0)
    y_kv(1, second).wait_recv()
    z_start("B", 1)
    for s in range(1, half):
        twin_q(s)
        own_q(s)
        for u in of(s):
            start(y_q(u, first))

    perm[...] = jnp.where(
        iota((GRAN, GRAN), 1) == perm_token(iota((GRAN, GRAN), 0)), 1.0, 0.0
    ).astype(BF16)
    origin = blk * block - wide
    shape = (GRAN, GRAN + 2 * REACH)
    token = perm_token(iota(shape, 0))
    for g in range(grans):
        q_at = wide + g * GRAN + token
        k_at = wide + g * GRAN - REACH + iota(shape, 1)
        ok = (jnp.abs(k_at - q_at) <= REACH) & (k_at + origin >= 0) & (k_at + origin < total)
        bias1[g] = jnp.where(ok, 0.0, MASK_FILL)
    per = FAR // NEAR
    shape = (per * rows, per * near_rows)
    row, col = iota(shape, 0), iota(shape, 1)
    q_at = (row % rows + side * FAR) * FAR + NEAR * (row // rows)
    k_at = (col % near_rows + (side - 1) * FAR) * FAR + NEAR * (col // near_rows)
    ok = (jnp.abs(k_at - q_at) <= REACH * NEAR) & (k_at + origin >= 0) & (k_at + origin < total)
    bias4[...] = jnp.where(ok, 0.0, MASK_FILL)
    shape = (rows, key_rows)
    q_at = iota(shape, 0) + side * FAR
    k_at = iota(shape, 1)
    ok = (
        (jnp.abs(k_at - q_at) <= REACH)
        & (k_at * FAR + origin >= 0)
        & (k_at * FAR + origin < total)
    )
    bias16[...] = jnp.where(ok, 0.0, MASK_FILL)

    def gather_keys(u, slot, chunks):
        for j in chunks:
            moved = jnp.dot(
                perm[...], kn[u, j * GRAN : (j + 1) * GRAN], preferred_element_type=F32
            )
            moved = moved.astype(BF16).reshape(FAR, FAR, 2 * HEAD_DIM)
            kp[slot, :, j * FAR : (j + 1) * FAR] = moved

    ends = tail // GRAN

    def attend_close(u):
        slot = u % 2
        y_q(u, second).wait_recv()
        gather_keys(u, slot, range(ends, span // GRAN - ends))
        for g in range(grans):
            moved = jnp.dot(
                perm[...], qn[u, g * GRAN : (g + 1) * GRAN], preferred_element_type=F32
            )
            moved = moved.astype(BF16)
            qp[slot, :, g * FAR : (g + 1) * FAR] = moved.reshape(FAR, FAR, HEAD_DIM)
            at = wide + g * GRAN - REACH
            k = kn[u, at : at + GRAN + 2 * REACH, :HEAD_DIM]
            v = kn[u, at : at + GRAN + 2 * REACH, HEAD_DIM:]
            sc = dot_t(moved, k) * scale + bias1[g]
            m = jnp.max(sc, axis=1, keepdims=True)
            p = jnp.exp2(sc - m)
            l = jnp.sum(p, axis=1, keepdims=True)
            o = jnp.dot(p.astype(BF16), v, preferred_element_type=F32)
            cut = (FAR, FAR, HEAD_DIM)
            o1[slot, :, g * FAR : (g + 1) * FAR] = o.reshape(cut)
            m1[slot, :, g * FAR : (g + 1) * FAR] = jnp.broadcast_to(m, o.shape).reshape(cut)
            l1[slot, :, g * FAR : (g + 1) * FAR] = jnp.broadcast_to(l, o.shape).reshape(cut)

    def attend_far(u):
        slot = u % 2
        s, h = u // heads, u % heads
        z_wait("T", u)
        gather_keys(u, slot, [*range(ends), *range(span // GRAN - ends, span // GRAN)])
        shuffle = perm[...]
        near_at = (side - 1) * FAR
        for group in range(NEAR):
            sel = slice(group * per, (group + 1) * per)
            flat = (per * rows, HEAD_DIM)
            q = qp[slot, sel].reshape(flat)
            k4 = kp[slot, sel, near_at : near_at + near_rows, :HEAD_DIM].reshape(-1, HEAD_DIM)
            v4 = kp[slot, sel, near_at : near_at + near_rows, HEAD_DIM:].reshape(-1, HEAD_DIM)
            s4 = dot_t(q, k4) * scale + bias4[...]
            b16 = bias16[...]
            s16 = jnp.concatenate(
                [
                    dot_t(qp[slot, group * per + i], kp[slot, group * per + i, :, :HEAD_DIM]) * scale + b16
                    for i in range(per)
                ],
                axis=0,
            )
            m_old = m1[slot, sel].reshape(flat)
            m_row = jnp.maximum(
                jnp.max(s4, axis=1, keepdims=True), jnp.max(s16, axis=1, keepdims=True)
            )
            m_new = jnp.maximum(m_old, m_row)
            m_col = m_new[:, :1]
            keep = jnp.exp2(m_old - m_new)
            p4 = jnp.exp2(s4 - m_col)
            p16 = jnp.exp2(s16 - m_col)
            l = l1[slot, sel].reshape(flat) * keep + (
                jnp.sum(p4, axis=1, keepdims=True) + jnp.sum(p16, axis=1, keepdims=True)
            )
            p16 = p16.astype(BF16)
            o16 = jnp.concatenate(
                [
                    jnp.dot(
                        p16[i * rows : (i + 1) * rows],
                        kp[slot, group * per + i, :, HEAD_DIM:],
                        preferred_element_type=F32,
                    )
                    for i in range(per)
                ],
                axis=0,
            )
            o = o1[slot, sel].reshape(flat) * keep + o16
            o = o + jnp.dot(p4.astype(BF16), v4, preferred_element_type=F32)
            mp[sel] = (o / l).astype(BF16).reshape(per, rows, HEAD_DIM)
            m1[slot, sel] = (m_new * LN2 + jnp.log(l)).reshape(per, rows, HEAD_DIM)
        lane = iota((GRAN, HEAD_DIM), 1)
        for g in range(grans):
            cut = slice(g * FAR, (g + 1) * FAR)
            back = lambda a: lax.dot_general(
                a, shuffle, (((0,), (0,)), ((), ())), preferred_element_type=F32
            )
            merged = lax.dot_general(
                shuffle,
                mp[:, cut].reshape(GRAN, HEAD_DIM),
                (((0,), (0,)), ((), ())),
                preferred_element_type=F32,
            )
            on[g * GRAN : (g + 1) * GRAN] = merged.astype(BF16)
            x = m1[slot, :, cut].reshape(GRAN, HEAD_DIM)
            high = x.astype(BF16).astype(F32)
            mid = (x - high).astype(BF16).astype(F32)
            low = x - high - mid
            terms = jnp.where(
                lane == 0, high, jnp.where(lane == 1, mid, jnp.where(lane == 2, low, 0.0))
            )
            lrow[:, g * GRAN : (g + 1) * GRAN] = jnp.sum(
                back(terms.astype(BF16)), axis=0, keepdims=True
            )
        outs[u] = on[pl.ds(second, length)]
        gath[t, mine + s, h] = on[pl.ds(first, length)]
        logs[mine + s, h] = lrow[:, pl.ds(first, length)]
        lsend[u] = lrow[:, pl.ds(second, length)]
        start(across(u, mine))
        start(piece("mr", u, t, mine, right))
        start(piece("ml", u, t, mine, left))
        start(log_across(u, mine))

    def across(u, base):
        return copy(
            ("yo", u), outs.at[u], gath.at[t, base + u // heads, u % heads], (twin, t)
        )

    def log_across(u, base):
        return copy(("yl", u), lsend.at[u], logs.at[base + u // heads, u % heads], (twin, t))

    def piece(name, u, owner, base, to):
        ref = gath.at[owner, base + u // heads, u % heads]
        return copy((name, u), ref, ref, (sp, to))

    def spread(u):
        across(u, other).wait_recv()
        start(piece("or", u, t, other, right))
        start(piece("ol", u, t, other, left))
        piece("mr", u, left, mine, right).wait_recv()
        start(piece("fr", u, left, mine, right))

    def spread_twin(u):
        piece("ol", u, right, other, left).wait_recv()
        start(piece("fl", u, right, other, left))
        log_across(u, other).wait_recv()

    def finish(j):
        acc = None
        square = None
        for n in range(gath.shape[0]):
            x = jnp.concatenate([gath[n, j, h] for h in range(heads)], axis=1).astype(F32)
            at = slice(n * cols, (n + 1) * cols)
            scaled = (x * gain[:, at]).astype(BF16)
            term = jnp.dot(scaled, wo[at], preferred_element_type=F32)
            sq = jnp.sum(x * x, axis=1, keepdims=True)
            acc = term if acc is None else acc + term
            square = sq if square is None else square + sq
        out[j] = (acc * lax.rsqrt(square / wo.shape[0] + NORM_FLOOR)).astype(BF16)

    def finish_mine(s):
        for u in of(s):
            piece("ml", u, right, mine, left).wait_recv()
            piece("fr", u, opposite, mine, right).wait_recv()
        finish(mine + s)

    def finish_other(s):
        for u in of(s):
            piece("or", u, left, other, right).wait_recv()
            piece("fl", u, opposite, other, left).wait_recv()
        finish(other + s)

    def arrived(u):
        z_wait("A", u)
        z_wait("B", u)

    arrived(0)
    z_start("T", 0)
    z_start("A", 2)
    arrived(1)
    z_start("T", 1)
    y_kv(2, second).wait_recv()
    z_start("B", 2)
    z_start("A", 3)
    attend_close(0)
    attend_far(0)
    attend_close(1)
    attend_far(1)
    arrived(2)
    z_start("T", 2)
    y_kv(3, second).wait_recv()
    z_start("B", 3)
    spread(0)
    spread(1)
    attend_close(2)
    spread_twin(0)
    spread_twin(1)
    got_wo.wait()
    arrived(3)
    z_start("T", 3)
    attend_close(3)
    attend_far(2)
    finish_mine(0)
    spread(2)
    attend_far(3)
    spread_twin(2)
    finish_other(0)
    spread(3)
    finish_mine(1)
    spread_twin(3)
    finish_other(1)
    for j in range(logs.shape[0]):
        for h in range(heads):
            log_out[j, h : h + 1] = logs[j, h]
    for c, there in sent:
        if there is None:
            c.wait_send()
        else:

            @pl.when(there)
            def _(c=c):
                c.wait_send()


def layer(nsp, ntp, tokens, wq, wk, wv, wo, tables, gain):
    seqs, length, width = tokens.shape
    half = seqs // 2
    cols = wq.shape[1]
    heads = cols // HEAD_DIM
    block = 2 * length
    wide = REACH * FAR
    span = block + 2 * wide
    rows = block // FAR
    near_rows = rows + 2 * FAR
    per = FAR // NEAR
    grans = block // GRAN
    hbm = pl.BlockSpec(memory_space=pl.ANY)
    vmem = pl.BlockSpec(memory_space=pltpu.VMEM)
    v = pltpu.VMEM
    return pl.pallas_call(
        functools.partial(layer_kernel, nsp),
        in_specs=[hbm] * 7 + [vmem] * 3,
        out_specs=[vmem, vmem],
        out_shape=[
            jax.ShapeDtypeStruct((seqs, length, wo.shape[1]), BF16),
            jax.ShapeDtypeStruct((seqs, heads, length), F32),
        ],
        scratch_shapes=[
            v(tokens.shape, BF16), v(wq.shape, BF16), v(wk.shape, BF16), v(wv.shape, BF16),
            v(wo.shape, BF16), v((length, HEAD_DIM), F32), v((length, HEAD_DIM), F32),
            v((half * heads, span, 2 * HEAD_DIM), BF16),
            v((half * heads, block, HEAD_DIM), BF16),
            v((half * heads, length, 2 * HEAD_DIM), BF16),
            v((half * heads, length, HEAD_DIM), BF16),
            v((ntp, seqs, heads, length, HEAD_DIM), BF16),
            v((half * heads, length, HEAD_DIM), BF16),
            v((seqs, heads, 1, length), F32),
            v((half * heads, 1, length), F32),
            v((1, block), F32),
            v((2, FAR, span // FAR, 2 * HEAD_DIM), BF16),
            v((2, FAR, rows, HEAD_DIM), BF16),
            v((FAR, rows, HEAD_DIM), BF16),
            v((block, HEAD_DIM), BF16),
            v((GRAN, GRAN), BF16),
            v((grans, GRAN, GRAN + 2 * REACH), F32),
            v((per * rows, per * near_rows), F32),
            v((rows, span // FAR), F32),
            v((2, FAR, rows, HEAD_DIM), F32),
            v((2, FAR, rows, HEAD_DIM), F32),
            v((2, FAR, rows, HEAD_DIM), F32),
            pltpu.SemaphoreType.DMA((seqs + 6,)),
            pltpu.SemaphoreType.DMA((16 * half * heads,)),
            pltpu.SemaphoreType.DMA((16 * half * heads,)),
        ],
        compiler_params=pltpu.CompilerParams(
            collective_id=0, has_side_effects=True, vmem_limit_bytes=56 * 2**20
        ),
        name="layer",
    )(tokens, wq, wk, wv, wo, *tables, gain)


def shards(tokens, query_weight, key_weight, value_weight, out_gain, out_weight):
    length = tokens.shape[1]
    nsp = lax.axis_size("sp")
    frequency = ROPE_BASE ** (-np.arange(HEAD_DIM // 2) / (HEAD_DIM // 2))
    frequency = np.tile(frequency, 2)[None, :]
    step = np.arange(length)[:, None] * frequency
    base = (np.arange(nsp) * length)[:, None] * frequency
    tables = [
        jnp.asarray(f(a).astype(np.float32)) for a in (step, base) for f in (np.cos, np.sin)
    ]
    return tuple(
        layer(
            nsp, lax.axis_size("tp"), tokens, query_weight, key_weight, value_weight,
            out_weight, tables, out_gain[None, :],
        )
    )


def solution(mesh):
    return jax.shard_map(
        shards,
        mesh=mesh,
        in_specs=(
            P(None, "sp", None),
            P(None, "tp"),
            P(None, "tp"),
            P(None, "tp"),
            P(),
            P(None, "tp"),
        ),
        out_specs=(P(None, "sp", "tp"), P(None, "tp", "sp")),
        check_vma=False,
    )
```

```python
import functools
import math

import jax
import jax.numpy as jnp
import numpy as np
from jax import lax
from jax.experimental import pallas as pl
from jax.experimental.pallas import tpu as pltpu
from jax.sharding import PartitionSpec as P

HEAD_DIM = 128
REACH = 64
FAR = 16
NEAR = 4
GRAN = FAR * FAR
ROPE_BASE = 10000.0
MASK_FILL = -1e30
NORM_FLOOR = 1e-06
LOG2E = 1.0 / math.log(2.0)
LN2 = math.log(2.0)
F32 = jnp.float32
BF16 = jnp.bfloat16

MESH = pl.DeviceIdType.MESH


def iota(shape, dim):
    return lax.broadcasted_iota(jnp.int32, shape, dim)


def perm_token(p):
    slot = p // FAR
    a = p % FAR
    residue = slot // NEAR + NEAR * (slot % (FAR // NEAR))
    return a * FAR + residue


def dot_t(a, b):
    return lax.dot_general(a, b, (((1,), (1,)), ((), ())), preferred_element_type=F32)


def layer_kernel(
    nsp, tok_h, wq_h, wk_h, wv_h, wo_h, cos_h, sin_h, cos_base, sin_base, gain,
    out, log_out,
    tok, wq, wk, wv, wo, cos, sin, kn, qn, kvs, qs, gath, outs, logs, lsend,
    kp, qp, mp, perm, bias1, bias4, bias16, o1, m1, l1, acc, sq,
    load_sem, send_sem, recv_sem,
):
    seqs, length = tok.shape[:2]
    block = 2 * length
    grans = block // GRAN
    wide = REACH * FAR
    side = wide // GRAN
    own = seqs // 2 * block
    span = own + 2 * wide
    window = block + 2 * wide
    rows = block // FAR
    key_rows = window // FAR
    near_rows = rows + 2 * FAR
    cols = wq.shape[1]
    heads = cols // HEAD_DIM
    total = nsp * length
    scale = HEAD_DIM**-0.5 * LOG2E
    sp, t = lax.axis_index("sp"), lax.axis_index("tp")
    plane = 2 * seqs
    z, y, c = sp // plane, (sp // 2) % seqs, sp % 2
    worker = y // 2
    mine = worker == c
    place = 2 * (y % 2) + c
    right, left, opposite = (t + 1) % 4, (t + 3) % 4, (t + 2) % 4
    part = 2 * z + c
    last = 2 * (nsp // plane) - 1
    above, below = part < last, part > 0

    def at(zz, yy, cc):
        return (zz * plane + yy * 2 + cc, t)

    def half_at(p):
        return at(p // 2, y, p % 2)

    def seq(k):
        return (y + k) % seqs

    loads = []

    def load(src, dst):
        copy = pltpu.make_async_copy(src, dst, load_sem.at[len(loads)])
        copy.start()
        loads.append(copy)
        return copy

    order = (1, 3, 2, 0)
    got_cos, got_sin = load(cos_h, cos), load(sin_h, sin)
    got_wk, got_wv = load(wk_h, wk), load(wv_h, wv)
    got_tok = {}
    for k in order[:1]:
        got_tok[k] = load(tok_h.at[seq(k)], tok.at[k])

    barrier = pltpu.get_barrier_semaphore()

    def greet(peer):
        pl.semaphore_signal(barrier, inc=1, device_id=peer, device_id_type=MESH)

    for k in range(1, seqs):
        greet(at(z, seq(k), worker))
    for i in range(2):
        for cc in range(2):

            @pl.when(jnp.logical_not((2 * c + i == y) & (cc == c)))
            def _(i=i, cc=cc):
                greet(at(z, 2 * c + i, cc))

    @pl.when(jnp.logical_not(mine))
    def _():
        greet(at(z, y, worker))

    greet((sp, right))
    greet((sp, left))

    @pl.when(above)
    def _():
        greet(half_at(part + 1))

    @pl.when(below)
    def _():
        greet(half_at(part - 1))

    count = (
        2 * seqs + 2 - 2 * mine.astype(jnp.int32)
        + above.astype(jnp.int32) + below.astype(jnp.int32)
    )

    @pl.when(jnp.logical_not(below))
    def _():
        for h in range(heads):
            kn[h, 0:wide] = jnp.zeros((wide, kn.shape[2]), BF16)

    @pl.when(jnp.logical_not(above))
    def _():
        for h in range(heads):
            kn[h, wide + own : span] = jnp.zeros((wide, kn.shape[2]), BF16)

    def copy(src, dst, send, recv, peer):
        return pltpu.make_async_remote_copy(
            src_ref=src, dst_ref=dst, send_sem=send_sem.at[send], recv_sem=recv_sem.at[recv],
            device_id=peer, device_id_type=MESH,
        )

    sent = []

    def start(c, there=None):
        if there is None:
            c.start()
        else:

            @pl.when(there)
            def _():
                c.start()

        sent.append((c, there))

    def unless(cond, c):
        @pl.when(jnp.logical_not(cond))
        def _():
            c.wait_recv()

    def chunk(j):
        return pl.ds(pl.multiple_of(wide + j * length, HEAD_DIM), length)

    def q_chunk(j):
        return pl.ds(pl.multiple_of(j * length, HEAD_DIM), length)

    def kv_copy(h, k, j):
        return copy(
            kvs.at[k * heads + h], kn.at[h, chunk(j)], h * 4 + k, h * 4 + j,
            at(z, seq(k), worker),
        )

    def q_copy(h, k, j):
        return copy(
            qs.at[k * heads + h], qn.at[h, q_chunk(j)], 8 + h * 4 + k, 8 + h * 4 + j,
            at(z, seq(k), worker),
        )

    def is_here(j):
        return (2 * c + j // 2 == y) & (j % 2 == c)

    def kv_send(h, k):
        if k == 0:

            @pl.when(mine)
            def _():
                kn[h, chunk(place)] = kvs[h]

        start(kv_copy(h, k, place), jnp.logical_not(mine) if k == 0 else None)

    def q_send(h, k):
        if k == 0:

            @pl.when(mine)
            def _():
                qn[h, q_chunk(place)] = qs[h]

        start(q_copy(h, k, place), jnp.logical_not(mine) if k == 0 else None)

    first_up = wide + own - wide
    cuts_up = [(first_up, 2 * length - (own - wide)), (wide + 2 * length, length), (wide + 3 * length, length)]
    cuts_down = [(wide, length), (wide + length, length), (wide + 2 * length, wide - 2 * length)]

    def up(h, p):
        row, size = cuts_up[p]
        return copy(
            kn.at[h, row : row + size], kn.at[h, row - own : row - own + size],
            16 + 3 * h + p, 16 + 3 * h + p, half_at(part + 1),
        )

    def down(h, p):
        row, size = cuts_down[p]
        return copy(
            kn.at[h, row : row + size], kn.at[h, row + own : row + own + size],
            22 + 3 * h + p, 22 + 3 * h + p, half_at(part - 1),
        )

    def forward(h):
        for j in range(4):
            unless(is_here(j), kv_copy(h, 0, j))
            if j < 3:
                start(down(h, j), below)
            if j > 0:
                start(up(h, j - 1), above)

    def halo(h):
        for p in range(3):
            unless(jnp.logical_not(below), up(h, p))
            unless(jnp.logical_not(above), down(h, p))

    def lanes(n):
        return slice(n * HEAD_DIM, (n + 1) * HEAD_DIM)

    def turned(x, w, store):
        a = jnp.dot(x, w[...], preferred_element_type=F32)
        for h in range(heads):
            one = a[:, lanes(h)]
            store(h, (one * cos[...] + pltpu.roll(one, HEAD_DIM // 2, 1) * sin[...]).astype(BF16))

    def project_kv(k):
        x = tok[k]

        def put(h, a):
            kvs[k * heads + h, :, :HEAD_DIM] = a

        turned(x, wk, put)
        v = jnp.dot(x, wv[...], preferred_element_type=F32).astype(BF16)
        for h in range(heads):
            kvs[k * heads + h, :, HEAD_DIM:] = v[:, lanes(h)]

    def project_q(k):
        def put(h, a):
            qs[k * heads + h] = a

        turned(tok[k], wq, put)

    cos_at, sin_at = cos_base[pl.ds(sp, 1)], sin_base[pl.ds(sp, 1)]
    sign = jnp.where(iota(cos.shape, 1) < HEAD_DIM // 2, -1.0, 1.0)
    got_cos.wait()
    got_sin.wait()
    cos_step, sin_step = cos[...], sin[...]
    cos[...] = cos_step * cos_at - sin_step * sin_at
    sin[...] = (sin_step * cos_at + cos_step * sin_at) * sign
    for c_ in (got_wk, got_wv, got_tok[order[0]]):
        c_.wait()
    for k in order[1:]:
        got_tok[k] = load(tok_h.at[seq(k)], tok.at[k])
    got_wq = load(wq_h, wq)
    got_wo = load(wo_h, wo)
    project_kv(order[0])
    pl.semaphore_wait(barrier, count)
    kv_send(0, order[0])
    for k in order[1:]:
        got_tok[k].wait()
        project_kv(k)
        kv_send(0, k)
    got_wq.wait()
    for k in order:
        project_q(k)
        q_send(0, k)
    for k in order:
        kv_send(1, k)
    for k in order:
        q_send(1, k)

    perm[...] = jnp.where(
        iota((GRAN, GRAN), 1) == perm_token(iota((GRAN, GRAN), 0)), 1.0, 0.0
    ).astype(BF16)
    per = FAR // NEAR
    for jb in range(2):
        origin = part * own - wide + jb * block
        shape = (GRAN, GRAN + 2 * REACH)
        token = perm_token(iota(shape, 0))
        for g in range(grans):
            q_at = wide + g * GRAN + token
            k_at = wide + g * GRAN - REACH + iota(shape, 1)
            ok = (jnp.abs(k_at - q_at) <= REACH) & (k_at + origin >= 0) & (k_at + origin < total)
            bias1[jb, g] = jnp.where(ok, 0.0, MASK_FILL)
        shape = (per * rows, per * near_rows)
        row, col = iota(shape, 0), iota(shape, 1)
        q_at = (row % rows + side * FAR) * FAR + NEAR * (row // rows)
        k_at = (col % near_rows + (side - 1) * FAR) * FAR + NEAR * (col // near_rows)
        ok = (jnp.abs(k_at - q_at) <= REACH * NEAR) & (k_at + origin >= 0) & (k_at + origin < total)
        bias4[jb] = jnp.where(ok, 0.0, MASK_FILL)
        shape = (rows, key_rows)
        q_at = iota(shape, 0) + side * FAR
        k_at = iota(shape, 1)
        ok = (
            (jnp.abs(k_at - q_at) <= REACH)
            & (k_at * FAR + origin >= 0)
            & (k_at * FAR + origin < total)
        )
        bias16[jb] = jnp.where(ok, 0.0, MASK_FILL)

    def gather_keys(h, chunks):
        for j in chunks:
            moved = jnp.dot(
                perm[...], kn[h, j * GRAN : (j + 1) * GRAN], preferred_element_type=F32
            )
            moved = moved.astype(BF16).reshape(FAR, FAR, 2 * HEAD_DIM)
            kp[h, :, j * FAR : (j + 1) * FAR] = moved

    def ready(h):
        gather_keys(h, range(side, (wide + own) // GRAN))
        for j in range(4):
            unless(is_here(j), q_copy(h, 0, j))
        halo(h)
        gather_keys(h, [*range(side), *range((wide + own) // GRAN, span // GRAN)])

    def attend_close(h, step):
        slot = step
        jb = (step + y) % 2
        off = jb * block
        for g in range(grans):
            moved = jnp.dot(
                perm[...],
                qn[h, pl.ds(pl.multiple_of(off + g * GRAN, GRAN), GRAN)],
                preferred_element_type=F32,
            )
            moved = moved.astype(BF16)
            qp[slot, :, g * FAR : (g + 1) * FAR] = moved.reshape(FAR, FAR, HEAD_DIM)
            near = pl.ds(
                pl.multiple_of(off + wide + g * GRAN - REACH, REACH), GRAN + 2 * REACH
            )
            k = kn[h, near, :HEAD_DIM]
            v = kn[h, near, HEAD_DIM:]
            sc = dot_t(moved, k) * scale + bias1[jb, g]
            m = jnp.max(sc, axis=1, keepdims=True)
            p = jnp.exp2(sc - m)
            l = jnp.sum(p, axis=1, keepdims=True)
            o = jnp.dot(p.astype(BF16), v, preferred_element_type=F32)
            cut = (FAR, FAR, HEAD_DIM)
            o1[slot, :, g * FAR : (g + 1) * FAR] = o.reshape(cut)
            m1[slot, :, g * FAR : (g + 1) * FAR] = jnp.broadcast_to(m, o.shape).reshape(cut)
            l1[slot, :, g * FAR : (g + 1) * FAR] = jnp.broadcast_to(l, o.shape).reshape(cut)

    def attend_far(h, step):
        slot = step
        hs = 2 * h + step
        jb = (step + y) % 2
        shuffle = perm[...]
        near = pl.ds(pl.multiple_of((side - 1) * FAR + jb * rows, FAR), near_rows)
        whole = pl.ds(pl.multiple_of(jb * rows, FAR), key_rows)
        for group in range(NEAR):
            sel = slice(group * per, (group + 1) * per)
            flat = (per * rows, HEAD_DIM)
            q = qp[slot, sel].reshape(flat)
            k4 = kp[h, sel, near, :HEAD_DIM].reshape(-1, HEAD_DIM)
            v4 = kp[h, sel, near, HEAD_DIM:].reshape(-1, HEAD_DIM)
            s4 = dot_t(q, k4) * scale + bias4[jb]
            b16 = bias16[jb]
            s16 = jnp.concatenate(
                [
                    dot_t(qp[slot, group * per + i], kp[h, group * per + i, whole, :HEAD_DIM]) * scale + b16
                    for i in range(per)
                ],
                axis=0,
            )
            m_old = m1[slot, sel].reshape(flat)
            m_row = jnp.maximum(
                jnp.max(s4, axis=1, keepdims=True), jnp.max(s16, axis=1, keepdims=True)
            )
            m_new = jnp.maximum(m_old, m_row)
            m_col = m_new[:, :1]
            keep = jnp.exp2(m_old - m_new)
            p4 = jnp.exp2(s4 - m_col)
            p16 = jnp.exp2(s16 - m_col)
            l = l1[slot, sel].reshape(flat) * keep + (
                jnp.sum(p4, axis=1, keepdims=True) + jnp.sum(p16, axis=1, keepdims=True)
            )
            p16 = p16.astype(BF16)
            o16 = jnp.concatenate(
                [
                    jnp.dot(
                        p16[i * rows : (i + 1) * rows],
                        kp[h, group * per + i, whole, HEAD_DIM:],
                        preferred_element_type=F32,
                    )
                    for i in range(per)
                ],
                axis=0,
            )
            o = o1[slot, sel].reshape(flat) * keep + o16
            o = o + jnp.dot(p4.astype(BF16), v4, preferred_element_type=F32)
            mp[slot, sel] = (o / l).astype(BF16).reshape(per, rows, HEAD_DIM)
            m1[slot, sel] = (m_new * LN2 + jnp.log(l)).reshape(per, rows, HEAD_DIM)
        lane = iota((GRAN, HEAD_DIM), 1)
        for g in range(grans):
            cut = slice(g * FAR, (g + 1) * FAR)
            back = lambda a: lax.dot_general(
                a, shuffle, (((0,), (0,)), ((), ())), preferred_element_type=F32
            )
            merged = lax.dot_general(
                shuffle,
                mp[slot, :, cut].reshape(GRAN, HEAD_DIM),
                (((0,), (0,)), ((), ())),
                preferred_element_type=F32,
            )
            outs[hs, g * GRAN : (g + 1) * GRAN] = merged.astype(BF16)
            x = m1[slot, :, cut].reshape(GRAN, HEAD_DIM)
            high = x.astype(BF16).astype(F32)
            mid = (x - high).astype(BF16).astype(F32)
            low = x - high - mid
            terms = jnp.where(
                lane == 0, high, jnp.where(lane == 1, mid, jnp.where(lane == 2, low, 0.0))
            )
            lsend[hs, :, g * GRAN : (g + 1) * GRAN] = jnp.sum(
                back(terms.astype(BF16)), axis=0, keepdims=True
            )
        for cc in range(2):
            home = 2 * c + jb
            here = (home == y) & (cc == c)
            cut = slice(cc * length, (cc + 1) * length)

            @pl.when(here)
            def _(cut=cut):
                gath[t, y, h] = outs[hs, cut]
                logs[y, h] = lsend[hs, :, cut]

            start(o_copy(h, y, outs.at[hs, cut], 2 * hs + cc, at(z, home, cc)), jnp.logical_not(here))
            start(l_copy(h, y, lsend.at[hs, :, cut], 2 * hs + cc, at(z, home, cc)), jnp.logical_not(here))

    def o_copy(h, s, src, n, peer):
        return copy(src, gath.at[t, s, h], 28 + n, 28 + 2 * s + h, peer)

    def l_copy(h, s, src, n, peer):
        return copy(src, logs.at[s, h], 36 + n, 36 + 2 * s + h, peer)

    def piece(kind, h, k, owner, to):
        ref = gath.at[owner, seq(k), h]
        n = 44 + 8 * kind + 2 * k + h
        return copy(ref, ref, n, n, (sp, to))

    def collect(h, k):
        w = o_copy(h, seq(k), outs.at[0, :length], 0, (sp, right))
        if k == 0:
            unless(mine, w)
        else:
            w.wait_recv()
        start(piece(0, h, k, t, right))
        start(piece(1, h, k, t, left))

    def relay(h, k):
        if k in (0, 1):
            piece(0, h, k, left, right).wait_recv()
            start(piece(2, h, k, left, right))
        else:
            piece(1, h, k, right, left).wait_recv()
            start(piece(2, h, k, right, left))

    def rest(h, k):
        if k in (0, 1):
            piece(1, h, k, right, left).wait_recv()
        else:
            piece(0, h, k, left, right).wait_recv()
        piece(2, h, k, opposite, right).wait_recv()

    def share(h, k):
        term, square = None, None
        s = seq(k)
        x = jnp.concatenate([gath[n, s, h] for n in range(4)], axis=1).astype(F32)
        at_ = [slice(n * cols + h * HEAD_DIM, n * cols + (h + 1) * HEAD_DIM) for n in range(4)]
        g = jnp.concatenate([gain[:, a] for a in at_], axis=1)
        w = jnp.concatenate([wo[a] for a in at_], axis=0)
        term = jnp.dot((x * g).astype(BF16), w, preferred_element_type=F32)
        return term, jnp.sum(x * x, axis=1, keepdims=True)

    def partial(h, k):
        rest(h, k)
        acc[k], sq[k] = share(h, k)

    def finish(h, k):
        rest(h, k)
        term, square = share(h, k)
        square = square + sq[k]
        out[seq(k)] = (
            (acc[k] + term) * lax.rsqrt(square / wo.shape[0] + NORM_FLOOR)
        ).astype(BF16)

    forward(0)
    ready(0)
    attend_close(0, 0)
    attend_far(0, 0)
    attend_close(0, 1)
    attend_far(0, 1)
    forward(1)
    for k in (0, 2):
        collect(0, k)
    for k in (0, 2):
        relay(0, k)
    for k in (1, 3):
        collect(0, k)
    for k in (1, 3):
        relay(0, k)
    ready(1)
    attend_close(1, 0)
    attend_far(1, 0)
    attend_close(1, 1)
    for k in (0, 2):
        collect(1, k)
    attend_far(1, 1)
    for k in (0, 2):
        relay(1, k)
    got_wo.wait()
    for k in (0, 2):
        partial(0, k)
    for k in (1, 3):
        collect(1, k)
    for k in (1, 3):
        partial(0, k)
    for k in (1, 3):
        relay(1, k)
    for k in (0, 2, 1, 3):
        finish(1, k)
    for k in range(seqs):
        for h in range(heads):
            w = l_copy(h, seq(k), lsend.at[0, :, :length], 0, (sp, right))
            if k == 0:
                unless(mine, w)
            else:
                w.wait_recv()
    for s in range(seqs):
        for h in range(heads):
            log_out[s, h : h + 1] = logs[s, h]
    for c_, there in sent:
        if there is None:
            c_.wait_send()
        else:

            @pl.when(there)
            def _(c_=c_):
                c_.wait_send()


def layer(nsp, ntp, tokens, wq, wk, wv, wo, tables, gain):
    seqs, length, width = tokens.shape
    cols = wq.shape[1]
    heads = cols // HEAD_DIM
    block = 2 * length
    wide = REACH * FAR
    own = seqs // 2 * block
    span = own + 2 * wide
    window = block + 2 * wide
    rows = block // FAR
    near_rows = rows + 2 * FAR
    per = FAR // NEAR
    grans = block // GRAN
    hbm = pl.BlockSpec(memory_space=pl.ANY)
    vmem = pl.BlockSpec(memory_space=pltpu.VMEM)
    v = pltpu.VMEM
    return pl.pallas_call(
        functools.partial(layer_kernel, nsp),
        in_specs=[hbm] * 7 + [vmem] * 3,
        out_specs=[vmem, vmem],
        out_shape=[
            jax.ShapeDtypeStruct((seqs, length, wo.shape[1]), BF16),
            jax.ShapeDtypeStruct((seqs, heads, length), F32),
        ],
        scratch_shapes=[
            v(tokens.shape, BF16), v(wq.shape, BF16), v(wk.shape, BF16), v(wv.shape, BF16),
            v(wo.shape, BF16), v((length, HEAD_DIM), F32), v((length, HEAD_DIM), F32),
            v((heads, span, 2 * HEAD_DIM), BF16),
            v((heads, own, HEAD_DIM), BF16),
            v((seqs * heads, length, 2 * HEAD_DIM), BF16),
            v((seqs * heads, length, HEAD_DIM), BF16),
            v((ntp, seqs, heads, length, HEAD_DIM), BF16),
            v((2 * heads, block, HEAD_DIM), BF16),
            v((seqs, heads, 1, length), F32),
            v((2 * heads, 1, block), F32),
            v((heads, FAR, span // FAR, 2 * HEAD_DIM), BF16),
            v((2, FAR, rows, HEAD_DIM), BF16),
            v((2, FAR, rows, HEAD_DIM), BF16),
            v((GRAN, GRAN), BF16),
            v((2, grans, GRAN, GRAN + 2 * REACH), F32),
            v((2, per * rows, per * near_rows), F32),
            v((2, rows, window // FAR), F32),
            v((2, FAR, rows, HEAD_DIM), F32),
            v((2, FAR, rows, HEAD_DIM), F32),
            v((2, FAR, rows, HEAD_DIM), F32),
            v((seqs, length, wo.shape[1]), F32),
            v((seqs, length, 1), F32),
            pltpu.SemaphoreType.DMA((seqs + 6,)),
            pltpu.SemaphoreType.DMA((68,)),
            pltpu.SemaphoreType.DMA((68,)),
        ],
        compiler_params=pltpu.CompilerParams(
            collective_id=0, has_side_effects=True, vmem_limit_bytes=56 * 2**20
        ),
        name="layer",
    )(tokens, wq, wk, wv, wo, *tables, gain)


def shards(tokens, query_weight, key_weight, value_weight, out_gain, out_weight):
    length = tokens.shape[1]
    nsp = lax.axis_size("sp")
    frequency = ROPE_BASE ** (-np.arange(HEAD_DIM // 2) / (HEAD_DIM // 2))
    frequency = np.tile(frequency, 2)[None, :]
    step = np.arange(length)[:, None] * frequency
    base = (np.arange(nsp) * length)[:, None] * frequency
    tables = [
        jnp.asarray(f(a).astype(np.float32)) for a in (step, base) for f in (np.cos, np.sin)
    ]
    return tuple(
        layer(
            nsp, lax.axis_size("tp"), tokens, query_weight, key_weight, value_weight,
            out_weight, tables, out_gain[None, :],
        )
    )


def solution(mesh):
    return jax.shard_map(
        shards,
        mesh=mesh,
        in_specs=(
            P(None, "sp", None),
            P(None, "tp"),
            P(None, "tp"),
            P(None, "tp"),
            P(),
            P(None, "tp"),
        ),
        out_specs=(P(None, "sp", "tp"), P(None, "tp", "sp")),
        check_vma=False,
    )
```

```python
import functools
import math

import jax
import jax.numpy as jnp
import numpy as np
from jax import lax
from jax.experimental import pallas as pl
from jax.experimental.pallas import tpu as pltpu
from jax.sharding import PartitionSpec as P

HEAD_DIM = 128
REACH = 64
FAR = 16
NEAR = 4
GRAN = FAR * FAR
ROPE_BASE = 10000.0
MASK_FILL = -1e30
NORM_FLOOR = 1e-06
LOG2E = 1.0 / math.log(2.0)
LN2 = math.log(2.0)
F32 = jnp.float32
BF16 = jnp.bfloat16

MESH = pl.DeviceIdType.MESH


def iota(shape, dim):
    return lax.broadcasted_iota(jnp.int32, shape, dim)


def perm_token(p):
    slot = p // FAR
    a = p % FAR
    residue = slot // NEAR + NEAR * (slot % (FAR // NEAR))
    return a * FAR + residue


def dot_t(a, b):
    return lax.dot_general(a, b, (((1,), (1,)), ((), ())), preferred_element_type=F32)


def layer_kernel(
    nsp, tok_h, wq_h, wk_h, wv_h, wo_h, cos_h, sin_h, cos_base, sin_base, gain,
    out, log_out,
    tok, wq, wkv, wo, cos, sin, kn, qn, kvs, qs, gath, outs, logs, lsend,
    kp, qp, mp, perm, bias1, bias4, bias16, o1, m1, l1, acc, sq,
    load_sem, send_sem, recv_sem,
):
    seqs, length = tok.shape[:2]
    block = 2 * length
    grans = block // GRAN
    wide = REACH * FAR
    side = wide // GRAN
    own = seqs // 2 * block
    span = own + 2 * wide
    window = block + 2 * wide
    rows = block // FAR
    key_rows = window // FAR
    near_rows = rows + 2 * FAR
    cols = wq.shape[1]
    heads = cols // HEAD_DIM
    ends = wide // GRAN
    stop = ends + own // GRAN
    total = nsp * length
    scale = HEAD_DIM**-0.5 * LOG2E
    sp, t = lax.axis_index("sp"), lax.axis_index("tp")
    plane = 2 * seqs
    z, y, c = sp // plane, (sp // 2) % seqs, sp % 2
    worker = y // 2
    mine = worker == c
    place = 2 * (y % 2) + c
    right, left, opposite = (t + 1) % 4, (t + 3) % 4, (t + 2) % 4
    part = 2 * z + c
    last = 2 * (nsp // plane) - 1
    above, below = part < last, part > 0

    def at(zz, yy, cc):
        return (zz * plane + yy * 2 + cc, t)

    def half_at(p):
        return at(p // 2, y, p % 2)

    def seq(k):
        return (y + k) % seqs

    loads = []

    def load(src, dst):
        copy = pltpu.make_async_copy(src, dst, load_sem.at[len(loads)])
        copy.start()
        loads.append(copy)
        return copy

    def lanes(n):
        return slice(n * HEAD_DIM, (n + 1) * HEAD_DIM)

    def load_kv(h):
        return (
            load(wk_h.at[:, lanes(h)], wkv.at[h, :, lanes(0)]),
            load(wv_h.at[:, lanes(h)], wkv.at[h, :, lanes(1)]),
        )

    def load_tok(k):
        return load(tok_h.at[seq(k)], tok.at[k])

    pairs = ((2, 0), (1, 3))
    got_rope = (load(cos_h, cos), load(sin_h, sin))
    got_first = (*load_kv(0), *[load_tok(k) for k in pairs[0]])
    got_second = [load_tok(k) for k in pairs[1]]
    got_wq = load(wq_h, wq)
    got_third = load_kv(1)
    got_wo = load(wo_h, wo)

    barrier = pltpu.get_barrier_semaphore()

    def greet(peer):
        pl.semaphore_signal(barrier, inc=1, device_id=peer, device_id_type=MESH)

    for k in range(1, seqs):
        greet(at(z, seq(k), worker))
    for i in range(2):
        for cc in range(2):

            @pl.when(jnp.logical_not((2 * c + i == y) & (cc == c)))
            def _(i=i, cc=cc):
                greet(at(z, 2 * c + i, cc))

    @pl.when(jnp.logical_not(mine))
    def _():
        greet(at(z, y, worker))

    greet((sp, right))
    greet((sp, left))

    @pl.when(above)
    def _():
        greet(half_at(part + 1))

    @pl.when(below)
    def _():
        greet(half_at(part - 1))

    count = (
        2 * seqs + 2 - 2 * mine.astype(jnp.int32)
        + above.astype(jnp.int32) + below.astype(jnp.int32)
    )

    @pl.when(jnp.logical_not(below))
    def _():
        for h in range(heads):
            kn[h, 0:wide] = jnp.zeros((wide, kn.shape[2]), BF16)

    @pl.when(jnp.logical_not(above))
    def _():
        for h in range(heads):
            kn[h, wide + own : span] = jnp.zeros((wide, kn.shape[2]), BF16)

    def copy(src, dst, send, recv, peer):
        return pltpu.make_async_remote_copy(
            src_ref=src, dst_ref=dst, send_sem=send_sem.at[send], recv_sem=recv_sem.at[recv],
            device_id=peer, device_id_type=MESH,
        )

    sent = []

    def start(c, there=None):
        if there is None:
            c.start()
        else:

            @pl.when(there)
            def _():
                c.start()

        sent.append((c, there))

    def unless(cond, c):
        @pl.when(jnp.logical_not(cond))
        def _():
            c.wait_recv()

    def chunk(j):
        return pl.ds(pl.multiple_of(wide + j * length, HEAD_DIM), length)

    def q_chunk(j):
        return pl.ds(pl.multiple_of(j * length, HEAD_DIM), length)

    def kv_copy(h, k, j):
        return copy(
            kvs.at[k * heads + h], kn.at[h, chunk(j)], h * 4 + k, h * 4 + j,
            at(z, seq(k), worker),
        )

    def q_copy(h, k, j):
        return copy(
            qs.at[k * heads + h], qn.at[h, q_chunk(j)], 8 + h * 4 + k, 8 + h * 4 + j,
            at(z, seq(k), worker),
        )

    def is_here(j):
        return (2 * c + j // 2 == y) & (j % 2 == c)

    def kv_send(h, k):
        if k == 0:

            @pl.when(mine)
            def _():
                kn[h, chunk(place)] = kvs[h]

        start(kv_copy(h, k, place), jnp.logical_not(mine) if k == 0 else None)

    def q_send(h, k):
        if k == 0:

            @pl.when(mine)
            def _():
                qn[h, q_chunk(place)] = qs[h]

        start(q_copy(h, k, place), jnp.logical_not(mine) if k == 0 else None)

    first_up = wide + own - wide
    cuts_up = [(first_up, 2 * length - (own - wide)), (wide + 2 * length, length), (wide + 3 * length, length)]
    cuts_down = [(wide, length), (wide + length, length), (wide + 2 * length, wide - 2 * length)]

    def up(h, p):
        row, size = cuts_up[p]
        return copy(
            kn.at[h, row : row + size], kn.at[h, row - own : row - own + size],
            16 + 3 * h + p, 16 + 3 * h + p, half_at(part + 1),
        )

    def down(h, p):
        row, size = cuts_down[p]
        return copy(
            kn.at[h, row : row + size], kn.at[h, row + own : row + own + size],
            22 + 3 * h + p, 22 + 3 * h + p, half_at(part - 1),
        )

    flip = y % 2 == 1

    def forward(h, far):
        def relay_in(js):
            for j in js:
                unless(is_here(j), kv_copy(h, 0, j))
                if j < 3:

                    @pl.when(below)
                    def _(j=j):
                        down(h, j).start()

                if j > 0:

                    @pl.when(above)
                    def _(j=j):
                        up(h, j - 1).start()

        @pl.when(flip != far)
        def _():
            relay_in((2, 3))

        @pl.when(flip == far)
        def _():
            relay_in((0, 1))

        if far:
            for p in range(3):
                sent.append((down(h, p), below))
                sent.append((up(h, p), above))

    def halo(h):
        for p in range(3):
            unless(jnp.logical_not(below), up(h, p))
            unless(jnp.logical_not(above), down(h, p))

    def turned(one):
        return (one * cos[...] + pltpu.roll(one, HEAD_DIM // 2, 1) * sin[...]).astype(BF16)

    def project_kv(h, ks):
        both = [jnp.dot(tok[k], wkv[h], preferred_element_type=F32) for k in ks]
        for k, a in zip(ks, both):
            kvs[k * heads + h, :, lanes(0)] = turned(a[:, lanes(0)])
            kvs[k * heads + h, :, lanes(1)] = a[:, lanes(1)].astype(BF16)

    def project_q(ks):
        both = [jnp.dot(tok[k], wq[...], preferred_element_type=F32) for k in ks]
        for k, a in zip(ks, both):
            for h in range(heads):
                qs[k * heads + h] = turned(a[:, lanes(h)])

    cos_at, sin_at = cos_base[pl.ds(sp, 1)], sin_base[pl.ds(sp, 1)]
    sign = jnp.where(iota(cos.shape, 1) < HEAD_DIM // 2, -1.0, 1.0)
    for c_ in got_rope:
        c_.wait()
    cos_step, sin_step = cos[...], sin[...]
    cos[...] = cos_step * cos_at - sin_step * sin_at
    sin[...] = (sin_step * cos_at + cos_step * sin_at) * sign
    for c_ in got_first:
        c_.wait()
    project_kv(0, pairs[0])
    pl.semaphore_wait(barrier, count)
    for k in pairs[0]:
        kv_send(0, k)
    for c_ in got_second:
        c_.wait()
    project_kv(0, pairs[1])
    for k in pairs[1]:
        kv_send(0, k)
    got_wq.wait()
    for ks in pairs:
        project_q(ks)
        for k in ks:
            q_send(0, k)
    for c_ in got_third:
        c_.wait()
    for ks in pairs:
        project_kv(1, ks)

    perm[...] = jnp.where(
        iota((GRAN, GRAN), 1) == perm_token(iota((GRAN, GRAN), 0)), 1.0, 0.0
    ).astype(BF16)
    per = FAR // NEAR
    for jb in range(2):
        origin = part * own - wide + jb * block
        shape = (GRAN, GRAN + 2 * REACH)
        token = perm_token(iota(shape, 0))
        for g in range(grans):
            q_at = wide + g * GRAN + token
            k_at = wide + g * GRAN - REACH + iota(shape, 1)
            ok = (jnp.abs(k_at - q_at) <= REACH) & (k_at + origin >= 0) & (k_at + origin < total)
            bias1[jb, g] = jnp.where(ok, 0.0, MASK_FILL)
        shape = (per * rows, per * near_rows)
        row, col = iota(shape, 0), iota(shape, 1)
        q_at = (row % rows + side * FAR) * FAR + NEAR * (row // rows)
        k_at = (col % near_rows + (side - 1) * FAR) * FAR + NEAR * (col // near_rows)
        ok = (jnp.abs(k_at - q_at) <= REACH * NEAR) & (k_at + origin >= 0) & (k_at + origin < total)
        bias4[jb] = jnp.where(ok, 0.0, MASK_FILL)
        shape = (rows, key_rows)
        q_at = iota(shape, 0) + side * FAR
        k_at = iota(shape, 1)
        ok = (
            (jnp.abs(k_at - q_at) <= REACH)
            & (k_at * FAR + origin >= 0)
            & (k_at * FAR + origin < total)
        )
        bias16[jb] = jnp.where(ok, 0.0, MASK_FILL)

    def gather_keys(h, chunks):
        for j in chunks:
            moved = jnp.dot(
                perm[...], kn[h, j * GRAN : (j + 1) * GRAN], preferred_element_type=F32
            )
            moved = moved.astype(BF16).reshape(FAR, FAR, 2 * HEAD_DIM)
            kp[h, :, j * FAR : (j + 1) * FAR] = moved

    def gather_own(h):
        gather_keys(h, range(ends, stop))

    def gather_ends(h):
        gather_keys(h, [*range(ends), *range(stop, span // GRAN)])

    def queries(h, step):
        for i in range(2):
            j = (step + y) % 2 * 2 + i
            unless(is_here(j), q_copy(h, 0, j))

    def close(h, step, g):
        jb = (step + y) % 2
        q_at = pl.multiple_of(jb * block + g * GRAN, GRAN)
        near = pl.ds(pl.multiple_of(q_at + wide - REACH, REACH), GRAN + 2 * REACH)
        sl = pl.ds(pl.multiple_of(g * FAR, FAR), FAR)
        moved = jnp.dot(perm[...], qn[h, pl.ds(q_at, GRAN)], preferred_element_type=F32)
        moved = moved.astype(BF16)
        qp[step, :, sl] = moved.reshape(FAR, FAR, HEAD_DIM)
        k = kn[h, near, lanes(0)]
        v = kn[h, near, lanes(1)]
        sc = dot_t(moved, k) * scale + bias1[jb, g]
        m = jnp.max(sc, axis=1, keepdims=True)
        p = jnp.exp2(sc - m)
        l = jnp.sum(p, axis=1, keepdims=True)
        o = jnp.dot(p.astype(BF16), v, preferred_element_type=F32)
        cut = (FAR, FAR, HEAD_DIM)
        o1[step, :, sl] = o.reshape(cut)
        m1[step, :, sl] = jnp.broadcast_to(m, o.shape).reshape(cut)
        l1[step, :, sl] = jnp.broadcast_to(l, o.shape).reshape(cut)

    def close_inner(h, step):
        for i in range(1, grans):
            close(h, step, i - (step + y) % 2)

    def close_outer(h, step):
        close(h, step, (step + y) % 2 * (grans - 1))

    def attend_far(h, step):
        slot = step
        hs = 2 * h + step
        jb = (step + y) % 2
        shuffle = perm[...]
        near = pl.ds(pl.multiple_of((side - 1) * FAR + jb * rows, FAR), near_rows)
        whole = pl.ds(pl.multiple_of(jb * rows, FAR), key_rows)
        for group in range(NEAR):
            sel = slice(group * per, (group + 1) * per)
            flat = (per * rows, HEAD_DIM)
            q = qp[slot, sel].reshape(flat)
            k4 = kp[h, sel, near, :HEAD_DIM].reshape(-1, HEAD_DIM)
            v4 = kp[h, sel, near, HEAD_DIM:].reshape(-1, HEAD_DIM)
            s4 = dot_t(q, k4) * scale + bias4[jb]
            b16 = bias16[jb]
            s16 = jnp.concatenate(
                [
                    dot_t(qp[slot, group * per + i], kp[h, group * per + i, whole, :HEAD_DIM]) * scale + b16
                    for i in range(per)
                ],
                axis=0,
            )
            m_old = m1[slot, sel].reshape(flat)
            m_row = jnp.maximum(
                jnp.max(s4, axis=1, keepdims=True), jnp.max(s16, axis=1, keepdims=True)
            )
            m_new = jnp.maximum(m_old, m_row)
            m_col = m_new[:, :1]
            keep = jnp.exp2(m_old - m_new)
            p4 = jnp.exp2(s4 - m_col)
            p16 = jnp.exp2(s16 - m_col)
            l = l1[slot, sel].reshape(flat) * keep + (
                jnp.sum(p4, axis=1, keepdims=True) + jnp.sum(p16, axis=1, keepdims=True)
            )
            p16 = p16.astype(BF16)
            o16 = jnp.concatenate(
                [
                    jnp.dot(
                        p16[i * rows : (i + 1) * rows],
                        kp[h, group * per + i, whole, HEAD_DIM:],
                        preferred_element_type=F32,
                    )
                    for i in range(per)
                ],
                axis=0,
            )
            o = o1[slot, sel].reshape(flat) * keep + o16
            o = o + jnp.dot(p4.astype(BF16), v4, preferred_element_type=F32)
            mp[slot, sel] = (o / l).astype(BF16).reshape(per, rows, HEAD_DIM)
            m1[slot, sel] = (m_new * LN2 + jnp.log(l)).reshape(per, rows, HEAD_DIM)
        lane = iota((GRAN, HEAD_DIM), 1)
        for g in range(grans):
            cut = slice(g * FAR, (g + 1) * FAR)
            back = lambda a: lax.dot_general(
                a, shuffle, (((0,), (0,)), ((), ())), preferred_element_type=F32
            )
            merged = lax.dot_general(
                shuffle,
                mp[slot, :, cut].reshape(GRAN, HEAD_DIM),
                (((0,), (0,)), ((), ())),
                preferred_element_type=F32,
            )
            outs[hs, g * GRAN : (g + 1) * GRAN] = merged.astype(BF16)
            x = m1[slot, :, cut].reshape(GRAN, HEAD_DIM)
            high = x.astype(BF16).astype(F32)
            mid = (x - high).astype(BF16).astype(F32)
            low = x - high - mid
            terms = jnp.where(
                lane == 0, high, jnp.where(lane == 1, mid, jnp.where(lane == 2, low, 0.0))
            )
            lsend[hs, :, g * GRAN : (g + 1) * GRAN] = jnp.sum(
                back(terms.astype(BF16)), axis=0, keepdims=True
            )
        for cc in range(2):
            home = 2 * c + jb
            here = (home == y) & (cc == c)
            cut = slice(cc * length, (cc + 1) * length)

            @pl.when(here)
            def _(cut=cut):
                gath[t, y, h] = outs[hs, cut]
                logs[y, h] = lsend[hs, :, cut]

            start(o_copy(h, y, outs.at[hs, cut], 2 * hs + cc, at(z, home, cc)), jnp.logical_not(here))
            start(l_copy(h, y, lsend.at[hs, :, cut], 2 * hs + cc, at(z, home, cc)), jnp.logical_not(here))

    def o_copy(h, s, src, n, peer):
        return copy(src, gath.at[t, s, h], 28 + n, 28 + 2 * s + h, peer)

    def l_copy(h, s, src, n, peer):
        return copy(src, logs.at[s, h], 36 + n, 36 + 2 * s + h, peer)

    def piece(kind, h, k, owner, to):
        ref = gath.at[owner, seq(k), h]
        n = 44 + 8 * kind + 2 * k + h
        return copy(ref, ref, n, n, (sp, to))

    def collect(h, *ks):
        for k in ks:
            o_copy(h, seq(k), outs.at[0, :length], 0, (sp, right)).wait_recv()
        for a, b in zip(ks, reversed(ks)):
            start(piece(0, h, a, t, right))
            start(piece(1, h, b, t, left))

    def spread(h):
        piece(0, h, 0, t, right).start()
        piece(1, h, 0, t, left).start()

    def collect_mine(h):
        @pl.when(mine)
        def _():
            spread(h)

    def collect_twin(h):
        @pl.when(jnp.logical_not(mine))
        def _():
            o_copy(h, y, outs.at[0, :length], 0, (sp, right)).wait_recv()
            spread(h)

        sent.append((piece(0, h, 0, t, right), None))
        sent.append((piece(1, h, 0, t, left), None))

    def relay(h, k):
        if k in (0, 1):
            piece(0, h, k, left, right).wait_recv()
            start(piece(2, h, k, left, right))
        else:
            piece(1, h, k, right, left).wait_recv()
            start(piece(2, h, k, right, left))

    def rest(h, k):
        if k in (0, 1):
            piece(1, h, k, right, left).wait_recv()
        else:
            piece(0, h, k, left, right).wait_recv()
        piece(2, h, k, opposite, right).wait_recv()

    def share(h, k):
        term, square = None, None
        s = seq(k)
        x = jnp.concatenate([gath[n, s, h] for n in range(4)], axis=1).astype(F32)
        at_ = [slice(n * cols + h * HEAD_DIM, n * cols + (h + 1) * HEAD_DIM) for n in range(4)]
        g = jnp.concatenate([gain[:, a] for a in at_], axis=1)
        w = jnp.concatenate([wo[a] for a in at_], axis=0)
        term = jnp.dot((x * g).astype(BF16), w, preferred_element_type=F32)
        return term, jnp.sum(x * x, axis=1, keepdims=True)

    def partial(h, k):
        rest(h, k)
        acc[k], sq[k] = share(h, k)

    def finish(h, k):
        rest(h, k)
        term, square = share(h, k)
        square = square + sq[k]
        out[seq(k)] = (
            (acc[k] + term) * lax.rsqrt(square / wo.shape[0] + NORM_FLOOR)
        ).astype(BF16)

    forward(0, False)
    forward(0, True)
    for k in pairs[0]:
        kv_send(1, k)
    for k in pairs[0]:
        q_send(1, k)
    for k in pairs[1]:
        kv_send(1, k)
    gather_own(0)
    queries(0, 0)
    close_inner(0, 0)
    halo(0)
    gather_ends(0)
    close_outer(0, 0)
    attend_far(0, 0)
    for k in pairs[1]:
        q_send(1, k)
    collect_mine(0)
    forward(1, False)
    queries(0, 1)
    close_inner(0, 1)
    close_outer(0, 1)
    attend_far(0, 1)
    collect_twin(0)
    forward(1, True)
    gather_own(1)
    queries(1, 0)
    close_inner(1, 0)
    collect(0, 2)
    relay(0, 0)
    halo(1)
    gather_ends(1)
    close_outer(1, 0)
    collect(0, 1, 3)
    attend_far(1, 0)
    relay(0, 2)
    collect_mine(1)
    queries(1, 1)
    close_inner(1, 1)
    close_outer(1, 1)
    relay(0, 1)
    attend_far(1, 1)
    relay(0, 3)
    collect_twin(1)
    collect(1, 2)
    got_wo.wait()
    partial(0, 0)
    relay(1, 0)
    partial(0, 2)
    collect(1, 1, 3)
    relay(1, 2)
    partial(0, 1)
    partial(0, 3)
    relay(1, 1)
    relay(1, 3)
    for k in (0, 2, 1, 3):
        finish(1, k)
    for k in range(seqs):
        for h in range(heads):
            w = l_copy(h, seq(k), lsend.at[0, :, :length], 0, (sp, right))
            if k == 0:
                unless(mine, w)
            else:
                w.wait_recv()
    for s in range(seqs):
        for h in range(heads):
            log_out[s, h : h + 1] = logs[s, h]
    for c_, there in sent:
        if there is None:
            c_.wait_send()
        else:

            @pl.when(there)
            def _(c_=c_):
                c_.wait_send()


def layer(nsp, ntp, tokens, wq, wk, wv, wo, tables, gain):
    seqs, length, width = tokens.shape
    cols = wq.shape[1]
    heads = cols // HEAD_DIM
    block = 2 * length
    wide = REACH * FAR
    own = seqs // 2 * block
    span = own + 2 * wide
    window = block + 2 * wide
    rows = block // FAR
    near_rows = rows + 2 * FAR
    per = FAR // NEAR
    grans = block // GRAN
    hbm = pl.BlockSpec(memory_space=pl.ANY)
    vmem = pl.BlockSpec(memory_space=pltpu.VMEM)
    v = pltpu.VMEM
    return pl.pallas_call(
        functools.partial(layer_kernel, nsp),
        in_specs=[hbm] * 7 + [vmem] * 3,
        out_specs=[vmem, vmem],
        out_shape=[
            v((seqs, length, wo.shape[1]), BF16),
            v((seqs, heads, length), F32),
        ],
        scratch_shapes=[
            v(tokens.shape, BF16), v(wq.shape, BF16), v((heads, width, 2 * HEAD_DIM), BF16),
            v(wo.shape, BF16), v((length, HEAD_DIM), F32), v((length, HEAD_DIM), F32),
            v((heads, span, 2 * HEAD_DIM), BF16),
            v((heads, own, HEAD_DIM), BF16),
            v((seqs * heads, length, 2 * HEAD_DIM), BF16),
            v((seqs * heads, length, HEAD_DIM), BF16),
            v((ntp, seqs, heads, length, HEAD_DIM), BF16),
            v((2 * heads, block, HEAD_DIM), BF16),
            v((seqs, heads, 1, length), F32),
            v((2 * heads, 1, block), F32),
            v((heads, FAR, span // FAR, 2 * HEAD_DIM), BF16),
            v((2, FAR, rows, HEAD_DIM), BF16),
            v((2, FAR, rows, HEAD_DIM), BF16),
            v((GRAN, GRAN), BF16),
            v((2, grans, GRAN, GRAN + 2 * REACH), F32),
            v((2, per * rows, per * near_rows), F32),
            v((2, rows, window // FAR), F32),
            v((2, FAR, rows, HEAD_DIM), F32),
            v((2, FAR, rows, HEAD_DIM), F32),
            v((2, FAR, rows, HEAD_DIM), F32),
            v((seqs, length, wo.shape[1]), F32),
            v((seqs, length, 1), F32),
            pltpu.SemaphoreType.DMA((seqs + 8,)),
            pltpu.SemaphoreType.DMA((68,)),
            pltpu.SemaphoreType.DMA((68,)),
        ],
        compiler_params=pltpu.CompilerParams(
            collective_id=0, has_side_effects=True, vmem_limit_bytes=56 * 2**20
        ),
        name="layer",
    )(tokens, wq, wk, wv, wo, *tables, gain)


def store_kernel(mixed, logs, mixed_out, log_out, sem):
    copies = [
        pltpu.make_async_copy(mixed.at[s], mixed_out.at[s], sem.at[s])
        for s in range(mixed.shape[0])
    ]
    copies.append(pltpu.make_async_copy(logs, log_out, sem.at[mixed.shape[0]]))
    for c in copies:
        c.start()
    for c in copies:
        c.wait()


def store(mixed, logs):
    hbm = pl.BlockSpec(memory_space=pl.ANY)
    vmem = pl.BlockSpec(memory_space=pltpu.VMEM)
    return pl.pallas_call(
        store_kernel,
        in_specs=[vmem] * 2,
        out_specs=[hbm] * 2,
        out_shape=[jax.ShapeDtypeStruct(a.shape, a.dtype) for a in (mixed, logs)],
        scratch_shapes=[pltpu.SemaphoreType.DMA((mixed.shape[0] + 1,))],
        compiler_params=pltpu.CompilerParams(vmem_limit_bytes=2**20),
        name="store",
    )(mixed, logs)


def shards(tokens, query_weight, key_weight, value_weight, out_gain, out_weight):
    length = tokens.shape[1]
    nsp = lax.axis_size("sp")
    frequency = ROPE_BASE ** (-np.arange(HEAD_DIM // 2) / (HEAD_DIM // 2))
    frequency = np.tile(frequency, 2)[None, :]
    step = np.arange(length)[:, None] * frequency
    base = (np.arange(nsp) * length)[:, None] * frequency
    tables = [
        jnp.asarray(f(a).astype(np.float32)) for a in (step, base) for f in (np.cos, np.sin)
    ]
    return tuple(
        store(*layer(
            nsp, lax.axis_size("tp"), tokens, query_weight, key_weight, value_weight,
            out_weight, tables, out_gain[None, :],
        ))
    )


def solution(mesh):
    return jax.shard_map(
        shards,
        mesh=mesh,
        in_specs=(
            P(None, "sp", None),
            P(None, "tp"),
            P(None, "tp"),
            P(None, "tp"),
            P(),
            P(None, "tp"),
        ),
        out_specs=(P(None, "sp", "tp"), P(None, "tp", "sp")),
        check_vma=False,
    )
```

```python
import functools
import math

import jax
import jax.numpy as jnp
import numpy as np
from jax import lax
from jax.experimental import pallas as pl
from jax.experimental.pallas import tpu as pltpu
from jax.sharding import PartitionSpec as P

HEAD_DIM = 128
REACH = 64
FAR = 16
NEAR = 4
GRAN = FAR * FAR
ROPE_BASE = 10000.0
MASK_FILL = -1e30
NORM_FLOOR = 1e-06
LOG2E = 1.0 / math.log(2.0)
LN2 = math.log(2.0)
F32 = jnp.float32
BF16 = jnp.bfloat16

MESH = pl.DeviceIdType.MESH


def iota(shape, dim):
    return lax.broadcasted_iota(jnp.int32, shape, dim)


def perm_token(p):
    slot = p // FAR
    a = p % FAR
    residue = slot // NEAR + NEAR * (slot % (FAR // NEAR))
    return a * FAR + residue


def dot_t(a, b):
    return lax.dot_general(a, b, (((1,), (1,)), ((), ())), preferred_element_type=F32)


def layer_kernel(
    nsp, tok_h, wq_h, wk_h, wv_h, wo_h, cos_h, sin_h, cos_base, sin_base, gain,
    out, log_out,
    tok, wq, wkv, wo, cos, sin, kn, qn, kvs, qs, gath, outs, logs, lsend,
    kp, qp, mp, perm, bias1, bias4, bias16, o1, m1, l1, acc, sq,
    load_sem, send_sem, recv_sem,
):
    seqs, length = tok.shape[:2]
    block = 2 * length
    grans = block // GRAN
    wide = REACH * FAR
    side = wide // GRAN
    own = seqs // 2 * block
    span = own + 2 * wide
    window = block + 2 * wide
    rows = block // FAR
    key_rows = window // FAR
    near_rows = rows + 2 * FAR
    cols = wq.shape[1]
    heads = cols // HEAD_DIM
    ends = wide // GRAN
    stop = ends + own // GRAN
    total = nsp * length
    scale = HEAD_DIM**-0.5 * LOG2E
    sp, t = lax.axis_index("sp"), lax.axis_index("tp")
    plane = 2 * seqs
    z, y, c = sp // plane, (sp // 2) % seqs, sp % 2
    worker = y // 2
    mine = worker == c
    place = 2 * (y % 2) + c
    right, left, opposite = (t + 1) % 4, (t + 3) % 4, (t + 2) % 4
    part = 2 * z + c
    last = 2 * (nsp // plane) - 1
    above, below = part < last, part > 0

    def at(zz, yy, cc):
        return (zz * plane + yy * 2 + cc, t)

    def half_at(p):
        return at(p // 2, y, p % 2)

    def seq(k):
        return (y + k) % seqs

    loads = []

    def load(src, dst):
        copy = pltpu.make_async_copy(src, dst, load_sem.at[len(loads)])
        copy.start()
        loads.append(copy)
        return copy

    def lanes(n):
        return slice(n * HEAD_DIM, (n + 1) * HEAD_DIM)

    def load_kv(h):
        return (
            load(wk_h.at[:, lanes(h)], wkv.at[h, :, lanes(0)]),
            load(wv_h.at[:, lanes(h)], wkv.at[h, :, lanes(1)]),
        )

    def load_tok(k):
        return load(tok_h.at[seq(k)], tok.at[k])

    pairs = ((2, 0), (1, 3))
    got_rope = (load(cos_h, cos), load(sin_h, sin))
    got_first = (*load_kv(0), load_tok(2))
    got_second = [load_tok(k) for k in pairs[1]]
    got_wq = (load(wq_h, wq), load_tok(0))
    got_third = load_kv(1)
    got_wo = load(wo_h, wo)

    barrier = pltpu.get_barrier_semaphore()

    def greet(peer):
        pl.semaphore_signal(barrier, inc=1, device_id=peer, device_id_type=MESH)

    for k in range(1, seqs):
        greet(at(z, seq(k), worker))
    for i in range(2):
        for cc in range(2):

            @pl.when(jnp.logical_not((2 * c + i == y) & (cc == c)))
            def _(i=i, cc=cc):
                greet(at(z, 2 * c + i, cc))

    @pl.when(jnp.logical_not(mine))
    def _():
        greet(at(z, y, worker))

    greet((sp, right))
    greet((sp, left))

    @pl.when(above)
    def _():
        greet(half_at(part + 1))

    @pl.when(below)
    def _():
        greet(half_at(part - 1))

    count = (
        2 * seqs + 2 - 2 * mine.astype(jnp.int32)
        + above.astype(jnp.int32) + below.astype(jnp.int32)
    )

    @pl.when(jnp.logical_not(below))
    def _():
        for h in range(heads):
            kn[h, 0:wide] = jnp.zeros((wide, kn.shape[2]), BF16)

    @pl.when(jnp.logical_not(above))
    def _():
        for h in range(heads):
            kn[h, wide + own : span] = jnp.zeros((wide, kn.shape[2]), BF16)

    def copy(src, dst, send, recv, peer):
        return pltpu.make_async_remote_copy(
            src_ref=src, dst_ref=dst, send_sem=send_sem.at[send], recv_sem=recv_sem.at[recv],
            device_id=peer, device_id_type=MESH,
        )

    sent = []

    def start(c, there=None):
        if there is None:
            c.start()
        else:

            @pl.when(there)
            def _():
                c.start()

        sent.append((c, there))

    def unless(cond, c):
        @pl.when(jnp.logical_not(cond))
        def _():
            c.wait_recv()

    def chunk(j):
        return pl.ds(pl.multiple_of(wide + j * length, HEAD_DIM), length)

    def q_chunk(j):
        return pl.ds(pl.multiple_of(j * length, HEAD_DIM), length)

    def kv_copy(h, k, j):
        return copy(
            kvs.at[k * heads + h], kn.at[h, chunk(j)], h * 4 + k, h * 4 + j,
            at(z, seq(k), worker),
        )

    def q_copy(h, k, j):
        return copy(
            qs.at[k * heads + h], qn.at[h, q_chunk(j)], 8 + h * 4 + k, 8 + h * 4 + j,
            at(z, seq(k), worker),
        )

    def is_here(j):
        return (2 * c + j // 2 == y) & (j % 2 == c)

    def kv_send(h, k):
        if k == 0:

            @pl.when(mine)
            def _():
                kn[h, chunk(place)] = kvs[h]

        start(kv_copy(h, k, place), jnp.logical_not(mine) if k == 0 else None)

    def q_send(h, k):
        if k == 0:

            @pl.when(mine)
            def _():
                qn[h, q_chunk(place)] = qs[h]

        start(q_copy(h, k, place), jnp.logical_not(mine) if k == 0 else None)

    first_up = wide + own - wide
    cuts_up = [(first_up, 2 * length - (own - wide)), (wide + 2 * length, length), (wide + 3 * length, length)]
    cuts_down = [(wide, length), (wide + length, length), (wide + 2 * length, wide - 2 * length)]

    def up(h, p):
        row, size = cuts_up[p]
        return copy(
            kn.at[h, row : row + size], kn.at[h, row - own : row - own + size],
            16 + 3 * h + p, 16 + 3 * h + p, half_at(part + 1),
        )

    def down(h, p):
        row, size = cuts_down[p]
        return copy(
            kn.at[h, row : row + size], kn.at[h, row + own : row + own + size],
            22 + 3 * h + p, 22 + 3 * h + p, half_at(part - 1),
        )

    flip = y % 2 == 1

    def forward(h, far):
        def relay_in(js):
            for j in js:
                unless(is_here(j), kv_copy(h, 0, j))
                if j < 3:

                    @pl.when(below)
                    def _(j=j):
                        down(h, j).start()

                if j > 0:

                    @pl.when(above)
                    def _(j=j):
                        up(h, j - 1).start()

        @pl.when(flip != far)
        def _():
            relay_in((2, 3))

        @pl.when(flip == far)
        def _():
            relay_in((0, 1))

        if far:
            for p in range(3):
                sent.append((down(h, p), below))
                sent.append((up(h, p), above))

    def halo(h):
        for p in range(3):
            unless(jnp.logical_not(below), up(h, p))
            unless(jnp.logical_not(above), down(h, p))

    def turned(one):
        return (one * cos[...] + pltpu.roll(one, HEAD_DIM // 2, 1) * sin[...]).astype(BF16)

    def store_kv(h, k, a):
        kvs[k * heads + h, :, lanes(0)] = turned(a[:, lanes(0)])
        kvs[k * heads + h, :, lanes(1)] = a[:, lanes(1)].astype(BF16)

    def project_kv(h, ks):
        both = [jnp.dot(tok[k], wkv[h], preferred_element_type=F32) for k in ks]
        for k, a in zip(ks, both):
            store_kv(h, k, a)

    def project_q(ks):
        both = [jnp.dot(tok[k], wq[...], preferred_element_type=F32) for k in ks]
        for k, a in zip(ks, both):
            for h in range(heads):
                qs[k * heads + h] = turned(a[:, lanes(h)])

    cos_at, sin_at = cos_base[pl.ds(sp, 1)], sin_base[pl.ds(sp, 1)]
    sign = jnp.where(iota(cos.shape, 1) < HEAD_DIM // 2, -1.0, 1.0)
    for c_ in got_rope:
        c_.wait()
    cos_step, sin_step = cos[...], sin[...]
    cos[...] = cos_step * cos_at - sin_step * sin_at
    sin[...] = (sin_step * cos_at + cos_step * sin_at) * sign
    for c_ in got_first:
        c_.wait()
    cut = length // 2
    halves = [
        jnp.dot(tok[2, i * cut : (i + 1) * cut], wkv[0], preferred_element_type=F32)
        for i in range(2)
    ]
    store_kv(0, 2, jnp.concatenate(halves, axis=0))
    pl.semaphore_wait(barrier, count)
    kv_send(0, 2)
    for c_ in got_second:
        c_.wait()
    project_kv(0, pairs[1])
    for k in pairs[1]:
        kv_send(0, k)
    for c_ in got_wq:
        c_.wait()
    halves = [
        jnp.dot(tok[0, i * cut : (i + 1) * cut], wkv[0], preferred_element_type=F32)
        for i in range(2)
    ]
    store_kv(0, 0, jnp.concatenate(halves, axis=0))
    kv_send(0, 0)
    for ks in pairs:
        project_q(ks)
        for k in ks:
            q_send(0, k)
    for c_ in got_third:
        c_.wait()
    for ks in pairs:
        project_kv(1, ks)

    perm[...] = jnp.where(
        iota((GRAN, GRAN), 1) == perm_token(iota((GRAN, GRAN), 0)), 1.0, 0.0
    ).astype(BF16)
    per = FAR // NEAR
    for jb in range(2):
        origin = part * own - wide + jb * block
        shape = (GRAN, GRAN + 2 * REACH)
        token = perm_token(iota(shape, 0))
        for g in range(grans):
            q_at = wide + g * GRAN + token
            k_at = wide + g * GRAN - REACH + iota(shape, 1)
            ok = (jnp.abs(k_at - q_at) <= REACH) & (k_at + origin >= 0) & (k_at + origin < total)
            bias1[jb, g] = jnp.where(ok, 0.0, MASK_FILL)
        shape = (per * rows, per * near_rows)
        row, col = iota(shape, 0), iota(shape, 1)
        q_at = (row % rows + side * FAR) * FAR + NEAR * (row // rows)
        k_at = (col % near_rows + (side - 1) * FAR) * FAR + NEAR * (col // near_rows)
        ok = (jnp.abs(k_at - q_at) <= REACH * NEAR) & (k_at + origin >= 0) & (k_at + origin < total)
        bias4[jb] = jnp.where(ok, 0.0, MASK_FILL)
        shape = (rows, key_rows)
        q_at = iota(shape, 0) + side * FAR
        k_at = iota(shape, 1)
        ok = (
            (jnp.abs(k_at - q_at) <= REACH)
            & (k_at * FAR + origin >= 0)
            & (k_at * FAR + origin < total)
        )
        bias16[jb] = jnp.where(ok, 0.0, MASK_FILL)

    def gather_keys(h, chunks):
        for j in chunks:
            moved = jnp.dot(
                perm[...], kn[h, j * GRAN : (j + 1) * GRAN], preferred_element_type=F32
            )
            moved = moved.astype(BF16).reshape(FAR, FAR, 2 * HEAD_DIM)
            kp[h, :, j * FAR : (j + 1) * FAR] = moved

    def gather_own(h):
        gather_keys(h, range(ends, stop))

    def gather_ends(h):
        gather_keys(h, [*range(ends), *range(stop, span // GRAN)])

    def queries(h, step):
        for i in range(2):
            j = (step + y) % 2 * 2 + i
            unless(is_here(j), q_copy(h, 0, j))

    def close(h, step, g):
        jb = (step + y) % 2
        q_at = pl.multiple_of(jb * block + g * GRAN, GRAN)
        near = pl.ds(pl.multiple_of(q_at + wide - REACH, REACH), GRAN + 2 * REACH)
        sl = pl.ds(pl.multiple_of(g * FAR, FAR), FAR)
        moved = jnp.dot(perm[...], qn[h, pl.ds(q_at, GRAN)], preferred_element_type=F32)
        moved = moved.astype(BF16)
        qp[step, :, sl] = moved.reshape(FAR, FAR, HEAD_DIM)
        k = kn[h, near, lanes(0)]
        v = kn[h, near, lanes(1)]
        sc = dot_t(moved, k) * scale + bias1[jb, g]
        m = jnp.max(sc, axis=1, keepdims=True)
        p = jnp.exp2(sc - m)
        l = jnp.sum(p, axis=1, keepdims=True)
        o = jnp.dot(p.astype(BF16), v, preferred_element_type=F32)
        cut = (FAR, FAR, HEAD_DIM)
        o1[step, :, sl] = o.reshape(cut)
        m1[step, :, sl] = jnp.broadcast_to(m, o.shape).reshape(cut)
        l1[step, :, sl] = jnp.broadcast_to(l, o.shape).reshape(cut)

    def close_inner(h, step):
        for i in range(1, grans):
            close(h, step, i - (step + y) % 2)

    def close_outer(h, step):
        close(h, step, (step + y) % 2 * (grans - 1))

    def attend_far(h, step, between=None):
        slot = step
        hs = 2 * h + step
        jb = (step + y) % 2
        shuffle = perm[...]
        near = pl.ds(pl.multiple_of((side - 1) * FAR + jb * rows, FAR), near_rows)
        whole = pl.ds(pl.multiple_of(jb * rows, FAR), key_rows)
        for group in range(NEAR):
            sel = slice(group * per, (group + 1) * per)
            flat = (per * rows, HEAD_DIM)
            q = qp[slot, sel].reshape(flat)
            k4 = kp[h, sel, near, :HEAD_DIM].reshape(-1, HEAD_DIM)
            v4 = kp[h, sel, near, HEAD_DIM:].reshape(-1, HEAD_DIM)
            s4 = dot_t(q, k4) * scale + bias4[jb]
            b16 = bias16[jb]
            s16 = jnp.concatenate(
                [
                    dot_t(qp[slot, group * per + i], kp[h, group * per + i, whole, :HEAD_DIM]) * scale + b16
                    for i in range(per)
                ],
                axis=0,
            )
            m_old = m1[slot, sel].reshape(flat)
            m_row = jnp.maximum(
                jnp.max(s4, axis=1, keepdims=True), jnp.max(s16, axis=1, keepdims=True)
            )
            m_new = jnp.maximum(m_old, m_row)
            m_col = m_new[:, :1]
            keep = jnp.exp2(m_old - m_new)
            p4 = jnp.exp2(s4 - m_col)
            p16 = jnp.exp2(s16 - m_col)
            l = l1[slot, sel].reshape(flat) * keep + (
                jnp.sum(p4, axis=1, keepdims=True) + jnp.sum(p16, axis=1, keepdims=True)
            )
            p16 = p16.astype(BF16)
            o16 = jnp.concatenate(
                [
                    jnp.dot(
                        p16[i * rows : (i + 1) * rows],
                        kp[h, group * per + i, whole, HEAD_DIM:],
                        preferred_element_type=F32,
                    )
                    for i in range(per)
                ],
                axis=0,
            )
            o = o1[slot, sel].reshape(flat) * keep + o16
            o = o + jnp.dot(p4.astype(BF16), v4, preferred_element_type=F32)
            if between is not None and group == NEAR // 2:
                between()
            mp[slot, sel] = (o / l).astype(BF16).reshape(per, rows, HEAD_DIM)
            m1[slot, sel] = (m_new * LN2 + jnp.log(l)).reshape(per, rows, HEAD_DIM)
        lane = iota((GRAN, HEAD_DIM), 1)
        for g in range(grans):
            cut = slice(g * FAR, (g + 1) * FAR)
            back = lambda a: lax.dot_general(
                a, shuffle, (((0,), (0,)), ((), ())), preferred_element_type=F32
            )
            merged = lax.dot_general(
                shuffle,
                mp[slot, :, cut].reshape(GRAN, HEAD_DIM),
                (((0,), (0,)), ((), ())),
                preferred_element_type=F32,
            )
            outs[hs, g * GRAN : (g + 1) * GRAN] = merged.astype(BF16)
            x = m1[slot, :, cut].reshape(GRAN, HEAD_DIM)
            high = x.astype(BF16).astype(F32)
            mid = (x - high).astype(BF16).astype(F32)
            low = x - high - mid
            terms = jnp.where(
                lane == 0, high, jnp.where(lane == 1, mid, jnp.where(lane == 2, low, 0.0))
            )
            lsend[hs, :, g * GRAN : (g + 1) * GRAN] = jnp.sum(
                back(terms.astype(BF16)), axis=0, keepdims=True
            )
        for cc in range(2):
            home = 2 * c + jb
            here = (home == y) & (cc == c)
            cut = slice(cc * length, (cc + 1) * length)

            @pl.when(here)
            def _(cut=cut):
                gath[t, y, h] = outs[hs, cut]
                logs[y, h] = lsend[hs, :, cut]

            start(o_copy(h, y, outs.at[hs, cut], 2 * hs + cc, at(z, home, cc)), jnp.logical_not(here))
            start(l_copy(h, y, lsend.at[hs, :, cut], 2 * hs + cc, at(z, home, cc)), jnp.logical_not(here))

    def o_copy(h, s, src, n, peer):
        return copy(src, gath.at[t, s, h], 28 + n, 28 + 2 * s + h, peer)

    def l_copy(h, s, src, n, peer):
        return copy(src, logs.at[s, h], 36 + n, 36 + 2 * s + h, peer)

    def piece(kind, h, k, owner, to):
        ref = gath.at[owner, seq(k), h]
        n = 44 + 8 * kind + 2 * k + h
        return copy(ref, ref, n, n, (sp, to))

    def collect(h, *ks):
        for k in ks:
            o_copy(h, seq(k), outs.at[0, :length], 0, (sp, right)).wait_recv()
        for a, b in zip(ks, reversed(ks)):
            start(piece(0, h, a, t, right))
            start(piece(1, h, b, t, left))

    def spread(h):
        piece(0, h, 0, t, right).start()
        piece(1, h, 0, t, left).start()

    def collect_mine(h):
        @pl.when(mine)
        def _():
            spread(h)

    def collect_twin(h):
        @pl.when(jnp.logical_not(mine))
        def _():
            o_copy(h, y, outs.at[0, :length], 0, (sp, right)).wait_recv()
            spread(h)

        sent.append((piece(0, h, 0, t, right), None))
        sent.append((piece(1, h, 0, t, left), None))

    def relay(h, k):
        if k in (0, 1):
            piece(0, h, k, left, right).wait_recv()
            start(piece(2, h, k, left, right))
        else:
            piece(1, h, k, right, left).wait_recv()
            start(piece(2, h, k, right, left))

    def rest(h, k):
        if k in (0, 1):
            piece(1, h, k, right, left).wait_recv()
        else:
            piece(0, h, k, left, right).wait_recv()
        piece(2, h, k, opposite, right).wait_recv()

    def share(h, k):
        term, square = None, None
        s = seq(k)
        x = jnp.concatenate([gath[n, s, h] for n in range(4)], axis=1).astype(F32)
        at_ = [slice(n * cols + h * HEAD_DIM, n * cols + (h + 1) * HEAD_DIM) for n in range(4)]
        g = jnp.concatenate([gain[:, a] for a in at_], axis=1)
        w = jnp.concatenate([wo[a] for a in at_], axis=0)
        term = jnp.dot((x * g).astype(BF16), w, preferred_element_type=F32)
        return term, jnp.sum(x * x, axis=1, keepdims=True)

    def partial(h, k):
        rest(h, k)
        acc[k], sq[k] = share(h, k)

    def finish(h, k):
        rest(h, k)
        term, square = share(h, k)
        square = square + sq[k]
        out[seq(k)] = (
            (acc[k] + term) * lax.rsqrt(square / wo.shape[0] + NORM_FLOOR)
        ).astype(BF16)

    forward(0, False)
    forward(0, True)
    for ks in pairs:
        for k in ks:
            kv_send(1, k)
    for k in pairs[0]:
        q_send(1, k)
    gather_own(0)
    queries(0, 0)
    close_inner(0, 0)
    halo(0)
    gather_ends(0)
    close_outer(0, 0)
    attend_far(0, 0)
    collect_mine(0)
    forward(1, False)
    queries(0, 1)
    close_inner(0, 1)
    close_outer(0, 1)

    def half_way():
        collect_twin(0)
        forward(1, True)

    attend_far(0, 1, half_way)
    for k in pairs[1]:
        q_send(1, k)
    gather_own(1)
    queries(1, 0)
    close_inner(1, 0)
    collect(0, 2)
    relay(0, 0)
    halo(1)
    gather_ends(1)
    close_outer(1, 0)
    collect(0, 1, 3)
    attend_far(1, 0)
    relay(0, 2)
    collect_mine(1)
    queries(1, 1)
    close_inner(1, 1)
    close_outer(1, 1)
    collect_twin(1)
    relay(0, 1)
    attend_far(1, 1, lambda: collect(1, 2))
    relay(0, 3)
    got_wo.wait()
    partial(0, 0)
    relay(1, 0)
    partial(0, 2)
    relay(1, 2)
    done = len(sent)
    collect(1, 1, 3)
    partial(0, 1)
    partial(0, 3)

    def settle(some):
        for c_, there in some:
            if there is None:
                c_.wait_send()
            else:

                @pl.when(there)
                def _(c_=c_):
                    c_.wait_send()

    settle(sent[:done])
    for k in range(seqs):
        for h in range(heads):
            w = l_copy(h, seq(k), lsend.at[0, :, :length], 0, (sp, right))
            if k == 0:
                unless(mine, w)
            else:
                w.wait_recv()
    for s in range(seqs):
        for h in range(heads):
            log_out[s, h : h + 1] = logs[s, h]
    relay(1, 1)
    relay(1, 3)
    for k in (0, 2, 1, 3):
        finish(1, k)
    settle(sent[done:])


def layer(nsp, ntp, tokens, wq, wk, wv, wo, tables, gain):
    seqs, length, width = tokens.shape
    cols = wq.shape[1]
    heads = cols // HEAD_DIM
    block = 2 * length
    wide = REACH * FAR
    own = seqs // 2 * block
    span = own + 2 * wide
    window = block + 2 * wide
    rows = block // FAR
    near_rows = rows + 2 * FAR
    per = FAR // NEAR
    grans = block // GRAN
    hbm = pl.BlockSpec(memory_space=pl.ANY)
    vmem = pl.BlockSpec(memory_space=pltpu.VMEM)
    v = pltpu.VMEM
    return pl.pallas_call(
        functools.partial(layer_kernel, nsp),
        in_specs=[hbm] * 7 + [vmem] * 3,
        out_specs=[vmem, vmem],
        out_shape=[
            v((seqs, length, wo.shape[1]), BF16),
            v((seqs, heads, length), F32),
        ],
        scratch_shapes=[
            v(tokens.shape, BF16), v(wq.shape, BF16), v((heads, width, 2 * HEAD_DIM), BF16),
            v(wo.shape, BF16), v((length, HEAD_DIM), F32), v((length, HEAD_DIM), F32),
            v((heads, span, 2 * HEAD_DIM), BF16),
            v((heads, own, HEAD_DIM), BF16),
            v((seqs * heads, length, 2 * HEAD_DIM), BF16),
            v((seqs * heads, length, HEAD_DIM), BF16),
            v((ntp, seqs, heads, length, HEAD_DIM), BF16),
            v((2 * heads, block, HEAD_DIM), BF16),
            v((seqs, heads, 1, length), F32),
            v((2 * heads, 1, block), F32),
            v((heads, FAR, span // FAR, 2 * HEAD_DIM), BF16),
            v((2, FAR, rows, HEAD_DIM), BF16),
            v((2, FAR, rows, HEAD_DIM), BF16),
            v((GRAN, GRAN), BF16),
            v((2, grans, GRAN, GRAN + 2 * REACH), F32),
            v((2, per * rows, per * near_rows), F32),
            v((2, rows, window // FAR), F32),
            v((2, FAR, rows, HEAD_DIM), F32),
            v((2, FAR, rows, HEAD_DIM), F32),
            v((2, FAR, rows, HEAD_DIM), F32),
            v((seqs, length, wo.shape[1]), F32),
            v((seqs, length, 1), F32),
            pltpu.SemaphoreType.DMA((seqs + 8,)),
            pltpu.SemaphoreType.DMA((68,)),
            pltpu.SemaphoreType.DMA((68,)),
        ],
        compiler_params=pltpu.CompilerParams(
            collective_id=0, has_side_effects=True, vmem_limit_bytes=56 * 2**20
        ),
        name="layer",
    )(tokens, wq, wk, wv, wo, *tables, gain)


def store_kernel(mixed, logs, mixed_out, log_out, sem):
    copies = [
        pltpu.make_async_copy(mixed.at[s], mixed_out.at[s], sem.at[s])
        for s in range(mixed.shape[0])
    ]
    copies.append(pltpu.make_async_copy(logs, log_out, sem.at[mixed.shape[0]]))
    for c in copies:
        c.start()
    for c in copies:
        c.wait()


def store(mixed, logs):
    hbm = pl.BlockSpec(memory_space=pl.ANY)
    vmem = pl.BlockSpec(memory_space=pltpu.VMEM)
    return pl.pallas_call(
        store_kernel,
        in_specs=[vmem] * 2,
        out_specs=[hbm] * 2,
        out_shape=[jax.ShapeDtypeStruct(a.shape, a.dtype) for a in (mixed, logs)],
        scratch_shapes=[pltpu.SemaphoreType.DMA((mixed.shape[0] + 1,))],
        compiler_params=pltpu.CompilerParams(vmem_limit_bytes=2**20),
        name="store",
    )(mixed, logs)


def shards(tokens, query_weight, key_weight, value_weight, out_gain, out_weight):
    length = tokens.shape[1]
    nsp = lax.axis_size("sp")
    frequency = ROPE_BASE ** (-np.arange(HEAD_DIM // 2) / (HEAD_DIM // 2))
    frequency = np.tile(frequency, 2)[None, :]
    step = np.arange(length)[:, None] * frequency
    base = (np.arange(nsp) * length)[:, None] * frequency
    tables = [
        jnp.asarray(f(a).astype(np.float32)) for a in (step, base) for f in (np.cos, np.sin)
    ]
    return tuple(
        store(*layer(
            nsp, lax.axis_size("tp"), tokens, query_weight, key_weight, value_weight,
            out_weight, tables, out_gain[None, :],
        ))
    )


def solution(mesh):
    return jax.shard_map(
        shards,
        mesh=mesh,
        in_specs=(
            P(None, "sp", None),
            P(None, "tp"),
            P(None, "tp"),
            P(None, "tp"),
            P(),
            P(None, "tp"),
        ),
        out_specs=(P(None, "sp", "tp"), P(None, "tp", "sp")),
        check_vma=False,
    )
```

```python
import functools
import math

import jax
import jax.numpy as jnp
import numpy as np
from jax import lax
from jax.experimental import pallas as pl
from jax.experimental.pallas import tpu as pltpu
from jax.sharding import PartitionSpec as P

HEAD_DIM = 128
REACH = 64
FAR = 16
NEAR = 4
GRAN = FAR * FAR
ROPE_BASE = 10000.0
MASK_FILL = -1e30
NORM_FLOOR = 1e-06
LOG2E = 1.0 / math.log(2.0)
LN2 = math.log(2.0)
F32 = jnp.float32
BF16 = jnp.bfloat16

MESH = pl.DeviceIdType.MESH


def iota(shape, dim):
    return lax.broadcasted_iota(jnp.int32, shape, dim)


def perm_token(p):
    slot = p // FAR
    a = p % FAR
    residue = slot // NEAR + NEAR * (slot % (FAR // NEAR))
    return a * FAR + residue


def dot_t(a, b):
    return lax.dot_general(a, b, (((1,), (1,)), ((), ())), preferred_element_type=F32)


def layer_kernel(
    nsp, tok_h, wq_h, wk_h, wv_h, wo_h, cos_h, sin_h, cos_base, sin_base, gain,
    out, log_out,
    tok, wq, wkv, wo, cos, sin, kn, qn, kvs, qs, gath, outs, logs, lsend,
    kp, qp, mp, perm, bias1, bias4, bias16, o1, m1, l1, acc, sq,
    load_sem, send_sem, recv_sem,
):
    seqs, length = tok.shape[:2]
    block = 2 * length
    grans = block // GRAN
    wide = REACH * FAR
    side = wide // GRAN
    own = seqs // 2 * block
    span = own + 2 * wide
    window = block + 2 * wide
    rows = block // FAR
    key_rows = window // FAR
    near_rows = rows + 2 * FAR
    cols = wq.shape[1]
    heads = cols // HEAD_DIM
    ends = wide // GRAN
    stop = ends + own // GRAN
    total = nsp * length
    scale = HEAD_DIM**-0.5 * LOG2E
    sp, t = lax.axis_index("sp"), lax.axis_index("tp")
    plane = 2 * seqs
    z, y, c = sp // plane, (sp // 2) % seqs, sp % 2
    worker = y // 2
    mine = worker == c
    place = 2 * (y % 2) + c
    right, left, opposite = (t + 1) % 4, (t + 3) % 4, (t + 2) % 4
    part = 2 * z + c
    last = 2 * (nsp // plane) - 1
    above, below = part < last, part > 0

    def at(zz, yy, cc):
        return (zz * plane + yy * 2 + cc, t)

    def half_at(p):
        return at(p // 2, y, p % 2)

    def seq(k):
        return (y + k) % seqs

    loads = []

    def load(src, dst):
        copy = pltpu.make_async_copy(src, dst, load_sem.at[len(loads)])
        copy.start()
        loads.append(copy)
        return copy

    def lanes(n):
        return slice(n * HEAD_DIM, (n + 1) * HEAD_DIM)

    def load_kv(h):
        return (
            load(wk_h.at[:, lanes(h)], wkv.at[h, :, lanes(0)]),
            load(wv_h.at[:, lanes(h)], wkv.at[h, :, lanes(1)]),
        )

    def load_tok(k):
        return load(tok_h.at[seq(k)], tok.at[k])

    pairs = ((2, 0), (1, 3))
    got_rope = (load(cos_h, cos), load(sin_h, sin))
    got_first = (*load_kv(0), load_tok(2))
    got_second = [load_tok(k) for k in pairs[1]]
    got_wq = (load(wq_h, wq), load_tok(0))
    got_third = load_kv(1)
    got_wo = load(wo_h, wo)

    barrier = pltpu.get_barrier_semaphore()

    def greet(peer):
        pl.semaphore_signal(barrier, inc=1, device_id=peer, device_id_type=MESH)

    for k in range(1, seqs):
        greet(at(z, seq(k), worker))
    for i in range(2):
        for cc in range(2):

            @pl.when(jnp.logical_not((2 * c + i == y) & (cc == c)))
            def _(i=i, cc=cc):
                greet(at(z, 2 * c + i, cc))

    @pl.when(jnp.logical_not(mine))
    def _():
        greet(at(z, y, worker))

    greet((sp, right))
    greet((sp, left))

    @pl.when(above)
    def _():
        greet(half_at(part + 1))

    @pl.when(below)
    def _():
        greet(half_at(part - 1))

    count = (
        2 * seqs + 2 - 2 * mine.astype(jnp.int32)
        + above.astype(jnp.int32) + below.astype(jnp.int32)
    )

    @pl.when(jnp.logical_not(below))
    def _():
        for h in range(heads):
            kn[h, 0:wide] = jnp.zeros((wide, kn.shape[2]), BF16)

    @pl.when(jnp.logical_not(above))
    def _():
        for h in range(heads):
            kn[h, wide + own : span] = jnp.zeros((wide, kn.shape[2]), BF16)

    def copy(src, dst, send, recv, peer):
        return pltpu.make_async_remote_copy(
            src_ref=src, dst_ref=dst, send_sem=send_sem.at[send], recv_sem=recv_sem.at[recv],
            device_id=peer, device_id_type=MESH,
        )

    sent = []

    def start(c, there=None):
        if there is None:
            c.start()
        else:

            @pl.when(there)
            def _():
                c.start()

        sent.append((c, there))

    def unless(cond, c):
        @pl.when(jnp.logical_not(cond))
        def _():
            c.wait_recv()

    def chunk(j):
        return pl.ds(pl.multiple_of(wide + j * length, HEAD_DIM), length)

    def q_chunk(j):
        return pl.ds(pl.multiple_of(j * length, HEAD_DIM), length)

    def kv_copy(h, k, j):
        return copy(
            kvs.at[k * heads + h], kn.at[h, chunk(j)], h * 4 + k, h * 4 + j,
            at(z, seq(k), worker),
        )

    def q_copy(h, k, j):
        return copy(
            qs.at[k * heads + h], qn.at[h, q_chunk(j)], 8 + h * 4 + k, 8 + h * 4 + j,
            at(z, seq(k), worker),
        )

    def is_here(j):
        return (2 * c + j // 2 == y) & (j % 2 == c)

    def kv_send(h, k):
        if k == 0:

            @pl.when(mine)
            def _():
                kn[h, chunk(place)] = kvs[h]

        start(kv_copy(h, k, place), jnp.logical_not(mine) if k == 0 else None)

    def q_send(h, k):
        if k == 0:

            @pl.when(mine)
            def _():
                qn[h, q_chunk(place)] = qs[h]

        start(q_copy(h, k, place), jnp.logical_not(mine) if k == 0 else None)

    first_up = wide + own - wide
    cuts_up = [(first_up, 2 * length - (own - wide)), (wide + 2 * length, length), (wide + 3 * length, length)]
    cuts_down = [(wide, length), (wide + length, length), (wide + 2 * length, wide - 2 * length)]

    def up(h, p):
        row, size = cuts_up[p]
        return copy(
            kn.at[h, row : row + size], kn.at[h, row - own : row - own + size],
            16 + 3 * h + p, 16 + 3 * h + p, half_at(part + 1),
        )

    def down(h, p):
        row, size = cuts_down[p]
        return copy(
            kn.at[h, row : row + size], kn.at[h, row + own : row + own + size],
            22 + 3 * h + p, 22 + 3 * h + p, half_at(part - 1),
        )

    flip = y % 2 == 1

    def forward(h, far):
        def relay_in(js):
            for j in js:
                unless(is_here(j), kv_copy(h, 0, j))
                if j < 3:

                    @pl.when(below)
                    def _(j=j):
                        down(h, j).start()

                if j > 0:

                    @pl.when(above)
                    def _(j=j):
                        up(h, j - 1).start()

        @pl.when(flip != far)
        def _():
            relay_in((2, 3))

        @pl.when(flip == far)
        def _():
            relay_in((0, 1))

        if far:
            for p in range(3):
                sent.append((down(h, p), below))
                sent.append((up(h, p), above))

    def halo(h):
        for p in range(3):
            unless(jnp.logical_not(below), up(h, p))
            unless(jnp.logical_not(above), down(h, p))

    def turned(one):
        return (one * cos[...] + pltpu.roll(one, HEAD_DIM // 2, 1) * sin[...]).astype(BF16)

    def store_kv(h, k, a):
        kvs[k * heads + h, :, lanes(0)] = turned(a[:, lanes(0)])
        kvs[k * heads + h, :, lanes(1)] = a[:, lanes(1)].astype(BF16)

    def project_kv(h, ks):
        both = [jnp.dot(tok[k], wkv[h], preferred_element_type=F32) for k in ks]
        for k, a in zip(ks, both):
            store_kv(h, k, a)

    def project_q(ks):
        both = [jnp.dot(tok[k], wq[...], preferred_element_type=F32) for k in ks]
        for k, a in zip(ks, both):
            for h in range(heads):
                qs[k * heads + h] = turned(a[:, lanes(h)])

    cos_at, sin_at = cos_base[pl.ds(sp, 1)], sin_base[pl.ds(sp, 1)]
    sign = jnp.where(iota(cos.shape, 1) < HEAD_DIM // 2, -1.0, 1.0)
    for c_ in got_rope:
        c_.wait()
    cos_step, sin_step = cos[...], sin[...]
    cos[...] = cos_step * cos_at - sin_step * sin_at
    sin[...] = (sin_step * cos_at + cos_step * sin_at) * sign
    for c_ in got_first:
        c_.wait()
    cut = length // 2
    halves = [
        jnp.dot(tok[2, i * cut : (i + 1) * cut], wkv[0], preferred_element_type=F32)
        for i in range(2)
    ]
    store_kv(0, 2, jnp.concatenate(halves, axis=0))
    pl.semaphore_wait(barrier, count)
    kv_send(0, 2)
    for c_ in got_second:
        c_.wait()
    project_kv(0, pairs[1])
    for k in pairs[1]:
        kv_send(0, k)
    for c_ in got_wq:
        c_.wait()
    halves = [
        jnp.dot(tok[0, i * cut : (i + 1) * cut], wkv[0], preferred_element_type=F32)
        for i in range(2)
    ]
    store_kv(0, 0, jnp.concatenate(halves, axis=0))
    kv_send(0, 0)
    for ks in pairs:
        project_q(ks)
        for k in ks:
            q_send(0, k)
    for c_ in got_third:
        c_.wait()
    for ks in pairs:
        project_kv(1, ks)

    forward(0, False)
    perm[...] = jnp.where(
        iota((GRAN, GRAN), 1) == perm_token(iota((GRAN, GRAN), 0)), 1.0, 0.0
    ).astype(BF16)
    per = FAR // NEAR
    for jb in range(2):
        origin = part * own - wide + jb * block
        shape = (GRAN, GRAN + 2 * REACH)
        token = perm_token(iota(shape, 0))
        for g in range(grans):
            q_at = wide + g * GRAN + token
            k_at = wide + g * GRAN - REACH + iota(shape, 1)
            ok = (jnp.abs(k_at - q_at) <= REACH) & (k_at + origin >= 0) & (k_at + origin < total)
            bias1[jb, g] = jnp.where(ok, 0.0, MASK_FILL)
        shape = (per * rows, per * near_rows)
        row, col = iota(shape, 0), iota(shape, 1)
        q_at = (row % rows + side * FAR) * FAR + NEAR * (row // rows)
        k_at = (col % near_rows + (side - 1) * FAR) * FAR + NEAR * (col // near_rows)
        ok = (jnp.abs(k_at - q_at) <= REACH * NEAR) & (k_at + origin >= 0) & (k_at + origin < total)
        bias4[jb] = jnp.where(ok, 0.0, MASK_FILL)
        shape = (rows, key_rows)
        q_at = iota(shape, 0) + side * FAR
        k_at = iota(shape, 1)
        ok = (
            (jnp.abs(k_at - q_at) <= REACH)
            & (k_at * FAR + origin >= 0)
            & (k_at * FAR + origin < total)
        )
        bias16[jb] = jnp.where(ok, 0.0, MASK_FILL)

    def gather_keys(h, chunks):
        for j in chunks:
            moved = jnp.dot(
                perm[...], kn[h, j * GRAN : (j + 1) * GRAN], preferred_element_type=F32
            )
            moved = moved.astype(BF16).reshape(FAR, FAR, 2 * HEAD_DIM)
            kp[h, :, j * FAR : (j + 1) * FAR] = moved

    def gather_own(h):
        gather_keys(h, range(ends, stop))

    def gather_ends(h):
        gather_keys(h, [*range(ends), *range(stop, span // GRAN)])

    def queries(h, step):
        for i in range(2):
            j = (step + y) % 2 * 2 + i
            unless(is_here(j), q_copy(h, 0, j))

    def close(h, step, g):
        jb = (step + y) % 2
        q_at = pl.multiple_of(jb * block + g * GRAN, GRAN)
        near = pl.ds(pl.multiple_of(q_at + wide - REACH, REACH), GRAN + 2 * REACH)
        sl = pl.ds(pl.multiple_of(g * FAR, FAR), FAR)
        moved = jnp.dot(perm[...], qn[h, pl.ds(q_at, GRAN)], preferred_element_type=F32)
        moved = moved.astype(BF16)
        qp[step, :, sl] = moved.reshape(FAR, FAR, HEAD_DIM)
        k = kn[h, near, lanes(0)]
        v = kn[h, near, lanes(1)]
        sc = dot_t(moved, k) * scale + bias1[jb, g]
        m = jnp.max(sc, axis=1, keepdims=True)
        p = jnp.exp2(sc - m)
        l = jnp.sum(p, axis=1, keepdims=True)
        o = jnp.dot(p.astype(BF16), v, preferred_element_type=F32)
        cut = (FAR, FAR, HEAD_DIM)
        o1[step, :, sl] = o.reshape(cut)
        m1[step, :, sl] = jnp.broadcast_to(m, o.shape).reshape(cut)
        l1[step, :, sl] = jnp.broadcast_to(l, o.shape).reshape(cut)

    def close_inner(h, step):
        for i in range(1, grans):
            close(h, step, i - (step + y) % 2)

    def close_outer(h, step):
        close(h, step, (step + y) % 2 * (grans - 1))

    def attend_far(h, step, between=None):
        slot = step
        hs = 2 * h + step
        jb = (step + y) % 2
        shuffle = perm[...]
        near = pl.ds(pl.multiple_of((side - 1) * FAR + jb * rows, FAR), near_rows)
        whole = pl.ds(pl.multiple_of(jb * rows, FAR), key_rows)
        for group in range(NEAR):
            sel = slice(group * per, (group + 1) * per)
            flat = (per * rows, HEAD_DIM)
            q = qp[slot, sel].reshape(flat)
            k4 = kp[h, sel, near, :HEAD_DIM].reshape(-1, HEAD_DIM)
            v4 = kp[h, sel, near, HEAD_DIM:].reshape(-1, HEAD_DIM)
            s4 = dot_t(q, k4) * scale + bias4[jb]
            b16 = bias16[jb]
            s16 = jnp.concatenate(
                [
                    dot_t(qp[slot, group * per + i], kp[h, group * per + i, whole, :HEAD_DIM]) * scale + b16
                    for i in range(per)
                ],
                axis=0,
            )
            m_old = m1[slot, sel].reshape(flat)
            m_row = jnp.maximum(
                jnp.max(s4, axis=1, keepdims=True), jnp.max(s16, axis=1, keepdims=True)
            )
            m_new = jnp.maximum(m_old, m_row)
            m_col = m_new[:, :1]
            keep = jnp.exp2(m_old - m_new)
            p4 = jnp.exp2(s4 - m_col)
            p16 = jnp.exp2(s16 - m_col)
            l = l1[slot, sel].reshape(flat) * keep + (
                jnp.sum(p4, axis=1, keepdims=True) + jnp.sum(p16, axis=1, keepdims=True)
            )
            p16 = p16.astype(BF16)
            o16 = jnp.concatenate(
                [
                    jnp.dot(
                        p16[i * rows : (i + 1) * rows],
                        kp[h, group * per + i, whole, HEAD_DIM:],
                        preferred_element_type=F32,
                    )
                    for i in range(per)
                ],
                axis=0,
            )
            o = o1[slot, sel].reshape(flat) * keep + o16
            o = o + jnp.dot(p4.astype(BF16), v4, preferred_element_type=F32)
            if between is not None and group == NEAR // 2:
                between()
            mp[slot, sel] = (o / l).astype(BF16).reshape(per, rows, HEAD_DIM)
            m1[slot, sel] = (m_new * LN2 + jnp.log(l)).reshape(per, rows, HEAD_DIM)
        lane = iota((GRAN, HEAD_DIM), 1)
        for g in range(grans):
            cut = slice(g * FAR, (g + 1) * FAR)
            back = lambda a: lax.dot_general(
                a, shuffle, (((0,), (0,)), ((), ())), preferred_element_type=F32
            )
            merged = lax.dot_general(
                shuffle,
                mp[slot, :, cut].reshape(GRAN, HEAD_DIM),
                (((0,), (0,)), ((), ())),
                preferred_element_type=F32,
            )
            outs[hs, g * GRAN : (g + 1) * GRAN] = merged.astype(BF16)
            x = m1[slot, :, cut].reshape(GRAN, HEAD_DIM)
            high = x.astype(BF16).astype(F32)
            mid = (x - high).astype(BF16).astype(F32)
            low = x - high - mid
            terms = jnp.where(
                lane == 0, high, jnp.where(lane == 1, mid, jnp.where(lane == 2, low, 0.0))
            )
            lsend[hs, :, g * GRAN : (g + 1) * GRAN] = jnp.sum(
                back(terms.astype(BF16)), axis=0, keepdims=True
            )
        for cc in range(2):
            home = 2 * c + jb
            here = (home == y) & (cc == c)
            cut = slice(cc * length, (cc + 1) * length)

            @pl.when(here)
            def _(cut=cut):
                gath[t, y, h] = outs[hs, cut]
                logs[y, h] = lsend[hs, :, cut]

            start(o_copy(h, y, outs.at[hs, cut], 2 * hs + cc, at(z, home, cc)), jnp.logical_not(here))
            start(l_copy(h, y, lsend.at[hs, :, cut], 2 * hs + cc, at(z, home, cc)), jnp.logical_not(here))

    def o_copy(h, s, src, n, peer):
        return copy(src, gath.at[t, s, h], 28 + n, 28 + 2 * s + h, peer)

    def l_copy(h, s, src, n, peer):
        return copy(src, logs.at[s, h], 36 + n, 36 + 2 * s + h, peer)

    def piece(kind, h, k, owner, to):
        ref = gath.at[owner, seq(k), h]
        n = 44 + 8 * kind + 2 * k + h
        return copy(ref, ref, n, n, (sp, to))

    def collect(h, *ks):
        for k in ks:
            o_copy(h, seq(k), outs.at[0, :length], 0, (sp, right)).wait_recv()
        for a, b in zip(ks, reversed(ks)):
            start(piece(0, h, a, t, right))
            start(piece(1, h, b, t, left))

    def spread(h):
        piece(0, h, 0, t, right).start()
        piece(1, h, 0, t, left).start()

    def collect_mine(h):
        @pl.when(mine)
        def _():
            spread(h)

    def collect_twin(h):
        @pl.when(jnp.logical_not(mine))
        def _():
            o_copy(h, y, outs.at[0, :length], 0, (sp, right)).wait_recv()
            spread(h)

        sent.append((piece(0, h, 0, t, right), None))
        sent.append((piece(1, h, 0, t, left), None))

    def relay(h, k):
        if k in (0, 1):
            piece(0, h, k, left, right).wait_recv()
            start(piece(2, h, k, left, right))
        else:
            piece(1, h, k, right, left).wait_recv()
            start(piece(2, h, k, right, left))

    def rest(h, k):
        if k in (0, 1):
            piece(1, h, k, right, left).wait_recv()
        else:
            piece(0, h, k, left, right).wait_recv()
        piece(2, h, k, opposite, right).wait_recv()

    def share(h, k):
        term, square = None, None
        s = seq(k)
        x = jnp.concatenate([gath[n, s, h] for n in range(4)], axis=1).astype(F32)
        at_ = [slice(n * cols + h * HEAD_DIM, n * cols + (h + 1) * HEAD_DIM) for n in range(4)]
        g = jnp.concatenate([gain[:, a] for a in at_], axis=1)
        w = jnp.concatenate([wo[a] for a in at_], axis=0)
        term = jnp.dot((x * g).astype(BF16), w, preferred_element_type=F32)
        return term, jnp.sum(x * x, axis=1, keepdims=True)

    def partial(h, k):
        rest(h, k)
        acc[k], sq[k] = share(h, k)

    def finish(h, k):
        rest(h, k)
        term, square = share(h, k)
        square = square + sq[k]
        out[seq(k)] = (
            (acc[k] + term) * lax.rsqrt(square / wo.shape[0] + NORM_FLOOR)
        ).astype(BF16)

    forward(0, True)
    for ks in pairs:
        for k in ks:
            kv_send(1, k)
    gather_own(0)
    queries(0, 0)
    close_inner(0, 0)
    halo(0)
    gather_ends(0)
    close_outer(0, 0)
    attend_far(0, 0)
    collect_mine(0)
    for k in pairs[0]:
        q_send(1, k)
    forward(1, False)
    queries(0, 1)
    close_inner(0, 1)
    close_outer(0, 1)

    def half_way():
        collect_twin(0)
        forward(1, True)

    attend_far(0, 1, half_way)
    for k in pairs[1]:
        q_send(1, k)
    gather_own(1)
    collect(0, 2)
    relay(0, 0)
    queries(1, 0)
    close_inner(1, 0)
    halo(1)
    gather_ends(1)
    close_outer(1, 0)
    collect(0, 1, 3)
    attend_far(1, 0)
    relay(0, 2)
    collect_mine(1)
    queries(1, 1)
    close_inner(1, 1)
    close_outer(1, 1)
    collect_twin(1)
    relay(0, 1)
    attend_far(1, 1, lambda: collect(1, 2))
    relay(0, 3)
    got_wo.wait()
    partial(0, 0)
    relay(1, 0)
    partial(0, 2)
    relay(1, 2)
    done = len(sent)
    collect(1, 1, 3)
    partial(0, 1)
    partial(0, 3)

    def settle(some):
        for c_, there in some:
            if there is None:
                c_.wait_send()
            else:

                @pl.when(there)
                def _(c_=c_):
                    c_.wait_send()

    settle(sent[:done])
    for k in range(seqs):
        for h in range(heads):
            w = l_copy(h, seq(k), lsend.at[0, :, :length], 0, (sp, right))
            if k == 0:
                unless(mine, w)
            else:
                w.wait_recv()
    for s in range(seqs):
        for h in range(heads):
            log_out[s, h : h + 1] = logs[s, h]
    relay(1, 1)
    relay(1, 3)
    for k in (0, 2, 1, 3):
        finish(1, k)
    settle(sent[done:])


def layer(nsp, ntp, tokens, wq, wk, wv, wo, tables, gain):
    seqs, length, width = tokens.shape
    cols = wq.shape[1]
    heads = cols // HEAD_DIM
    block = 2 * length
    wide = REACH * FAR
    own = seqs // 2 * block
    span = own + 2 * wide
    window = block + 2 * wide
    rows = block // FAR
    near_rows = rows + 2 * FAR
    per = FAR // NEAR
    grans = block // GRAN
    hbm = pl.BlockSpec(memory_space=pl.ANY)
    vmem = pl.BlockSpec(memory_space=pltpu.VMEM)
    v = pltpu.VMEM
    return pl.pallas_call(
        functools.partial(layer_kernel, nsp),
        in_specs=[hbm] * 7 + [vmem] * 3,
        out_specs=[vmem, vmem],
        out_shape=[
            v((seqs, length, wo.shape[1]), BF16),
            v((seqs, heads, length), F32),
        ],
        scratch_shapes=[
            v(tokens.shape, BF16), v(wq.shape, BF16), v((heads, width, 2 * HEAD_DIM), BF16),
            v(wo.shape, BF16), v((length, HEAD_DIM), F32), v((length, HEAD_DIM), F32),
            v((heads, span, 2 * HEAD_DIM), BF16),
            v((heads, own, HEAD_DIM), BF16),
            v((seqs * heads, length, 2 * HEAD_DIM), BF16),
            v((seqs * heads, length, HEAD_DIM), BF16),
            v((ntp, seqs, heads, length, HEAD_DIM), BF16),
            v((2 * heads, block, HEAD_DIM), BF16),
            v((seqs, heads, 1, length), F32),
            v((2 * heads, 1, block), F32),
            v((heads, FAR, span // FAR, 2 * HEAD_DIM), BF16),
            v((2, FAR, rows, HEAD_DIM), BF16),
            v((2, FAR, rows, HEAD_DIM), BF16),
            v((GRAN, GRAN), BF16),
            v((2, grans, GRAN, GRAN + 2 * REACH), F32),
            v((2, per * rows, per * near_rows), F32),
            v((2, rows, window // FAR), F32),
            v((2, FAR, rows, HEAD_DIM), F32),
            v((2, FAR, rows, HEAD_DIM), F32),
            v((2, FAR, rows, HEAD_DIM), F32),
            v((seqs, length, wo.shape[1]), F32),
            v((seqs, length, 1), F32),
            pltpu.SemaphoreType.DMA((seqs + 8,)),
            pltpu.SemaphoreType.DMA((68,)),
            pltpu.SemaphoreType.DMA((68,)),
        ],
        compiler_params=pltpu.CompilerParams(
            collective_id=0, has_side_effects=True, vmem_limit_bytes=56 * 2**20
        ),
        name="layer",
    )(tokens, wq, wk, wv, wo, *tables, gain)


def store_kernel(mixed, logs, mixed_out, log_out, sem):
    copies = [
        pltpu.make_async_copy(mixed.at[s], mixed_out.at[s], sem.at[s])
        for s in range(mixed.shape[0])
    ]
    copies.append(pltpu.make_async_copy(logs, log_out, sem.at[mixed.shape[0]]))
    for c in copies:
        c.start()
    for c in copies:
        c.wait()


def store(mixed, logs):
    hbm = pl.BlockSpec(memory_space=pl.ANY)
    vmem = pl.BlockSpec(memory_space=pltpu.VMEM)
    return pl.pallas_call(
        store_kernel,
        in_specs=[vmem] * 2,
        out_specs=[hbm] * 2,
        out_shape=[jax.ShapeDtypeStruct(a.shape, a.dtype) for a in (mixed, logs)],
        scratch_shapes=[pltpu.SemaphoreType.DMA((mixed.shape[0] + 1,))],
        compiler_params=pltpu.CompilerParams(vmem_limit_bytes=2**20),
        name="store",
    )(mixed, logs)


def shards(tokens, query_weight, key_weight, value_weight, out_gain, out_weight):
    length = tokens.shape[1]
    nsp = lax.axis_size("sp")
    frequency = ROPE_BASE ** (-np.arange(HEAD_DIM // 2) / (HEAD_DIM // 2))
    frequency = np.tile(frequency, 2)[None, :]
    step = np.arange(length)[:, None] * frequency
    base = (np.arange(nsp) * length)[:, None] * frequency
    tables = [
        jnp.asarray(f(a).astype(np.float32)) for a in (step, base) for f in (np.cos, np.sin)
    ]
    return tuple(
        store(*layer(
            nsp, lax.axis_size("tp"), tokens, query_weight, key_weight, value_weight,
            out_weight, tables, out_gain[None, :],
        ))
    )


def solution(mesh):
    return jax.shard_map(
        shards,
        mesh=mesh,
        in_specs=(
            P(None, "sp", None),
            P(None, "tp"),
            P(None, "tp"),
            P(None, "tp"),
            P(),
            P(None, "tp"),
        ),
        out_specs=(P(None, "sp", "tp"), P(None, "tp", "sp")),
        check_vma=False,
    )
```

```python
import functools
import math

import jax
import jax.numpy as jnp
import numpy as np
from jax import lax
from jax.experimental import pallas as pl
from jax.experimental.pallas import tpu as pltpu
from jax.sharding import PartitionSpec as P

HEAD_DIM = 128
REACH = 64
FAR = 16
NEAR = 4
GRAN = FAR * FAR
ROPE_BASE = 10000.0
MASK_FILL = -1e30
NORM_FLOOR = 1e-06
LOG2E = 1.0 / math.log(2.0)
LN2 = math.log(2.0)
F32 = jnp.float32
BF16 = jnp.bfloat16

MESH = pl.DeviceIdType.MESH


def iota(shape, dim):
    return lax.broadcasted_iota(jnp.int32, shape, dim)


def perm_token(p):
    slot = p // FAR
    a = p % FAR
    residue = slot // NEAR + NEAR * (slot % (FAR // NEAR))
    return a * FAR + residue


def dot_t(a, b):
    return lax.dot_general(a, b, (((1,), (1,)), ((), ())), preferred_element_type=F32)


def layer_kernel(
    nsp, tok_h, wq_h, wk_h, wv_h, wo_h, cos_h, sin_h, cos_base, sin_base, gain,
    out, log_out,
    tok, wq, wkv, wo, cos, sin, kn, qn, kvs, qs, gath, outs, logs, lsend,
    kp, qp, mp, perm, bias1, bias4, bias16, o1, m1, l1, acc, sq,
    load_sem, send_sem, recv_sem,
):
    seqs, length = tok.shape[:2]
    block = 2 * length
    grans = block // GRAN
    wide = REACH * FAR
    side = wide // GRAN
    own = seqs // 2 * block
    span = own + 2 * wide
    window = block + 2 * wide
    rows = block // FAR
    key_rows = window // FAR
    near_rows = rows + 2 * FAR
    cols = wq.shape[1]
    heads = cols // HEAD_DIM
    ends = wide // GRAN
    stop = ends + own // GRAN
    total = nsp * length
    scale = HEAD_DIM**-0.5 * LOG2E
    sp, t = lax.axis_index("sp"), lax.axis_index("tp")
    plane = 2 * seqs
    z, y, c = sp // plane, (sp // 2) % seqs, sp % 2
    worker = y // 2
    mine = worker == c
    place = 2 * (y % 2) + c
    right, left, opposite = (t + 1) % 4, (t + 3) % 4, (t + 2) % 4
    part = 2 * z + c
    last = 2 * (nsp // plane) - 1
    above, below = part < last, part > 0

    def at(zz, yy, cc):
        return (zz * plane + yy * 2 + cc, t)

    def half_at(p):
        return at(p // 2, y, p % 2)

    def seq(k):
        return (y + k) % seqs

    loads = []

    def load(src, dst):
        copy = pltpu.make_async_copy(src, dst, load_sem.at[len(loads)])
        copy.start()
        loads.append(copy)
        return copy

    def lanes(n):
        return slice(n * HEAD_DIM, (n + 1) * HEAD_DIM)

    def load_kv(h):
        return (
            load(wk_h.at[:, lanes(h)], wkv.at[h, :, lanes(0)]),
            load(wv_h.at[:, lanes(h)], wkv.at[h, :, lanes(1)]),
        )

    def load_tok(k):
        return load(tok_h.at[seq(k)], tok.at[k])

    pairs = ((2, 0), (1, 3))
    got_rope = (load(cos_h, cos), load(sin_h, sin))
    got_first = (*load_kv(0), load_tok(2))
    got_second = [load_tok(k) for k in pairs[1]]
    got_wq = (load(wq_h, wq), load_tok(0))
    got_third = load_kv(1)
    got_wo = load(wo_h, wo)

    barrier = pltpu.get_barrier_semaphore()

    def greet(peer):
        pl.semaphore_signal(barrier, inc=1, device_id=peer, device_id_type=MESH)

    for k in range(1, seqs):
        greet(at(z, seq(k), worker))
    for i in range(2):
        for cc in range(2):

            @pl.when(jnp.logical_not((2 * c + i == y) & (cc == c)))
            def _(i=i, cc=cc):
                greet(at(z, 2 * c + i, cc))

    @pl.when(jnp.logical_not(mine))
    def _():
        greet(at(z, y, worker))

    greet((sp, right))
    greet((sp, left))

    @pl.when(above)
    def _():
        greet(half_at(part + 1))

    @pl.when(below)
    def _():
        greet(half_at(part - 1))

    count = (
        2 * seqs + 2 - 2 * mine.astype(jnp.int32)
        + above.astype(jnp.int32) + below.astype(jnp.int32)
    )

    @pl.when(jnp.logical_not(below))
    def _():
        for h in range(heads):
            kn[h, 0:wide] = jnp.zeros((wide, kn.shape[2]), BF16)

    @pl.when(jnp.logical_not(above))
    def _():
        for h in range(heads):
            kn[h, wide + own : span] = jnp.zeros((wide, kn.shape[2]), BF16)

    def copy(src, dst, send, recv, peer):
        return pltpu.make_async_remote_copy(
            src_ref=src, dst_ref=dst, send_sem=send_sem.at[send], recv_sem=recv_sem.at[recv],
            device_id=peer, device_id_type=MESH,
        )

    sent = []

    def start(c, there=None):
        if there is None:
            c.start()
        else:

            @pl.when(there)
            def _():
                c.start()

        sent.append((c, there))

    def unless(cond, c):
        @pl.when(jnp.logical_not(cond))
        def _():
            c.wait_recv()

    def chunk(j):
        return pl.ds(pl.multiple_of(wide + j * length, HEAD_DIM), length)

    def q_chunk(j):
        return pl.ds(pl.multiple_of(j * length, HEAD_DIM), length)

    piece_rows = length // 2

    def kv_copy(h, k, j, i):
        at_ = pl.ds(pl.multiple_of(wide + j * length + i * piece_rows, REACH), piece_rows)
        n = 68 * i + h * 4
        return copy(
            kvs.at[k * heads + h, pl.ds(i * piece_rows, piece_rows)], kn.at[h, at_], n + k, n + j,
            at(z, seq(k), worker),
        )

    def q_copy(h, k, j):
        return copy(
            qs.at[k * heads + h], qn.at[h, q_chunk(j)], 8 + h * 4 + k, 8 + h * 4 + j,
            at(z, seq(k), worker),
        )

    def is_here(j):
        return (2 * c + j // 2 == y) & (j % 2 == c)

    def kv_send(h, k):
        if k == 0:

            @pl.when(mine)
            def _():
                kn[h, chunk(place)] = kvs[h]

        for i in range(2):
            start(kv_copy(h, k, place, i), jnp.logical_not(mine) if k == 0 else None)

    def q_send(h, k):
        if k == 0:

            @pl.when(mine)
            def _():
                qn[h, q_chunk(place)] = qs[h]

        start(q_copy(h, k, place), jnp.logical_not(mine) if k == 0 else None)

    spans = [(max(n * piece_rows, own - wide), (n + 1) * piece_rows) for n in range(8)]
    cuts_up = [(wide + a, b - a) for a, b in spans if b > a]
    spans = [(n * piece_rows, min((n + 1) * piece_rows, wide)) for n in range(8)]
    cuts_down = [(wide + a, b - a) for a, b in spans if b > a]

    def up(h, p):
        row, size = cuts_up[p]
        return copy(
            kn.at[h, row : row + size], kn.at[h, row - own : row - own + size],
            76 + 6 * h + p, 76 + 6 * h + p, half_at(part + 1),
        )

    def down(h, p):
        row, size = cuts_down[p]
        return copy(
            kn.at[h, row : row + size], kn.at[h, row + own : row + own + size],
            88 + 6 * h + p, 88 + 6 * h + p, half_at(part - 1),
        )

    flip = y % 2 == 1

    def forward(h, far):
        def relay_in(js):
            for n in [2 * j + i for j in js for i in range(2)]:
                unless(is_here(n // 2), kv_copy(h, 0, n // 2, n % 2))
                if n < 6:

                    @pl.when(below)
                    def _(n=n):
                        down(h, n).start()

                if n > 1:

                    @pl.when(above)
                    def _(n=n):
                        up(h, n - 2).start()

        @pl.when(flip != far)
        def _():
            relay_in((2, 3))

        @pl.when(flip == far)
        def _():
            relay_in((0, 1))

        if far:
            for p in range(6):
                sent.append((down(h, p), below))
                sent.append((up(h, p), above))

    def halo(h):
        for p in range(6):
            unless(jnp.logical_not(below), up(h, p))
            unless(jnp.logical_not(above), down(h, p))

    def turned(one):
        return (one * cos[...] + pltpu.roll(one, HEAD_DIM // 2, 1) * sin[...]).astype(BF16)

    def store_kv(h, k, a):
        kvs[k * heads + h, :, lanes(0)] = turned(a[:, lanes(0)])
        kvs[k * heads + h, :, lanes(1)] = a[:, lanes(1)].astype(BF16)

    def project_kv(h, ks):
        both = [jnp.dot(tok[k], wkv[h], preferred_element_type=F32) for k in ks]
        for k, a in zip(ks, both):
            store_kv(h, k, a)

    def project_q(ks):
        both = [jnp.dot(tok[k], wq[...], preferred_element_type=F32) for k in ks]
        for k, a in zip(ks, both):
            for h in range(heads):
                qs[k * heads + h] = turned(a[:, lanes(h)])

    cos_at, sin_at = cos_base[pl.ds(sp, 1)], sin_base[pl.ds(sp, 1)]
    sign = jnp.where(iota(cos.shape, 1) < HEAD_DIM // 2, -1.0, 1.0)
    for c_ in got_rope:
        c_.wait()
    cos_step, sin_step = cos[...], sin[...]
    cos[...] = cos_step * cos_at - sin_step * sin_at
    sin[...] = (sin_step * cos_at + cos_step * sin_at) * sign
    for c_ in got_first:
        c_.wait()
    cut = length // 2
    halves = [
        jnp.dot(tok[2, i * cut : (i + 1) * cut], wkv[0], preferred_element_type=F32)
        for i in range(2)
    ]
    store_kv(0, 2, jnp.concatenate(halves, axis=0))
    pl.semaphore_wait(barrier, count)
    kv_send(0, 2)
    for c_ in got_second:
        c_.wait()
    project_kv(0, pairs[1])
    for k in pairs[1]:
        kv_send(0, k)
    for c_ in got_wq:
        c_.wait()
    halves = [
        jnp.dot(tok[0, i * cut : (i + 1) * cut], wkv[0], preferred_element_type=F32)
        for i in range(2)
    ]
    store_kv(0, 0, jnp.concatenate(halves, axis=0))
    kv_send(0, 0)
    for ks in pairs:
        project_q(ks)
        for k in ks:
            q_send(0, k)
    for c_ in got_third:
        c_.wait()
    for ks in pairs:
        project_kv(1, ks)

    forward(0, False)
    perm[...] = jnp.where(
        iota((GRAN, GRAN), 1) == perm_token(iota((GRAN, GRAN), 0)), 1.0, 0.0
    ).astype(BF16)
    per = FAR // NEAR
    for jb in range(2):
        origin = part * own - wide + jb * block
        shape = (GRAN, GRAN + 2 * REACH)
        token = perm_token(iota(shape, 0))
        for g in range(grans):
            q_at = wide + g * GRAN + token
            k_at = wide + g * GRAN - REACH + iota(shape, 1)
            ok = (jnp.abs(k_at - q_at) <= REACH) & (k_at + origin >= 0) & (k_at + origin < total)
            bias1[jb, g] = jnp.where(ok, 0.0, MASK_FILL)
        shape = (per * rows, per * near_rows)
        row, col = iota(shape, 0), iota(shape, 1)
        q_at = (row % rows + side * FAR) * FAR + NEAR * (row // rows)
        k_at = (col % near_rows + (side - 1) * FAR) * FAR + NEAR * (col // near_rows)
        ok = (jnp.abs(k_at - q_at) <= REACH * NEAR) & (k_at + origin >= 0) & (k_at + origin < total)
        bias4[jb] = jnp.where(ok, 0.0, MASK_FILL)
        shape = (rows, key_rows)
        q_at = iota(shape, 0) + side * FAR
        k_at = iota(shape, 1)
        ok = (
            (jnp.abs(k_at - q_at) <= REACH)
            & (k_at * FAR + origin >= 0)
            & (k_at * FAR + origin < total)
        )
        bias16[jb] = jnp.where(ok, 0.0, MASK_FILL)

    def gather_keys(h, chunks):
        for j in chunks:
            moved = jnp.dot(
                perm[...], kn[h, j * GRAN : (j + 1) * GRAN], preferred_element_type=F32
            )
            moved = moved.astype(BF16).reshape(FAR, FAR, 2 * HEAD_DIM)
            kp[h, :, j * FAR : (j + 1) * FAR] = moved

    def gather_own(h):
        gather_keys(h, range(ends, stop))

    def gather_ends(h):
        gather_keys(h, [*range(ends), *range(stop, span // GRAN)])

    def queries(h, step):
        for i in range(2):
            j = (step + y) % 2 * 2 + i
            unless(is_here(j), q_copy(h, 0, j))

    def close(h, step, g):
        jb = (step + y) % 2
        q_at = pl.multiple_of(jb * block + g * GRAN, GRAN)
        near = pl.ds(pl.multiple_of(q_at + wide - REACH, REACH), GRAN + 2 * REACH)
        sl = pl.ds(pl.multiple_of(g * FAR, FAR), FAR)
        moved = jnp.dot(perm[...], qn[h, pl.ds(q_at, GRAN)], preferred_element_type=F32)
        moved = moved.astype(BF16)
        qp[step, :, sl] = moved.reshape(FAR, FAR, HEAD_DIM)
        k = kn[h, near, lanes(0)]
        v = kn[h, near, lanes(1)]
        sc = dot_t(moved, k) * scale + bias1[jb, g]
        m = jnp.max(sc, axis=1, keepdims=True)
        p = jnp.exp2(sc - m)
        l = jnp.sum(p, axis=1, keepdims=True)
        o = jnp.dot(p.astype(BF16), v, preferred_element_type=F32)
        cut = (FAR, FAR, HEAD_DIM)
        o1[step, :, sl] = o.reshape(cut)
        m1[step, :, sl] = jnp.broadcast_to(m, o.shape).reshape(cut)
        l1[step, :, sl] = jnp.broadcast_to(l, o.shape).reshape(cut)

    def close_inner(h, step):
        for i in range(1, grans):
            close(h, step, i - (step + y) % 2)

    def close_outer(h, step):
        close(h, step, (step + y) % 2 * (grans - 1))

    def attend_far(h, step, between=None):
        slot = step
        hs = 2 * h + step
        jb = (step + y) % 2
        shuffle = perm[...]
        near = pl.ds(pl.multiple_of((side - 1) * FAR + jb * rows, FAR), near_rows)
        whole = pl.ds(pl.multiple_of(jb * rows, FAR), key_rows)
        for group in range(NEAR):
            sel = slice(group * per, (group + 1) * per)
            flat = (per * rows, HEAD_DIM)
            q = qp[slot, sel].reshape(flat)
            k4 = kp[h, sel, near, :HEAD_DIM].reshape(-1, HEAD_DIM)
            v4 = kp[h, sel, near, HEAD_DIM:].reshape(-1, HEAD_DIM)
            s4 = dot_t(q, k4) * scale + bias4[jb]
            b16 = bias16[jb]
            s16 = jnp.concatenate(
                [
                    dot_t(qp[slot, group * per + i], kp[h, group * per + i, whole, :HEAD_DIM]) * scale + b16
                    for i in range(per)
                ],
                axis=0,
            )
            m_old = m1[slot, sel].reshape(flat)
            m_row = jnp.maximum(
                jnp.max(s4, axis=1, keepdims=True), jnp.max(s16, axis=1, keepdims=True)
            )
            m_new = jnp.maximum(m_old, m_row)
            m_col = m_new[:, :1]
            keep = jnp.exp2(m_old - m_new)
            p4 = jnp.exp2(s4 - m_col)
            p16 = jnp.exp2(s16 - m_col)
            l = l1[slot, sel].reshape(flat) * keep + (
                jnp.sum(p4, axis=1, keepdims=True) + jnp.sum(p16, axis=1, keepdims=True)
            )
            p16 = p16.astype(BF16)
            o16 = jnp.concatenate(
                [
                    jnp.dot(
                        p16[i * rows : (i + 1) * rows],
                        kp[h, group * per + i, whole, HEAD_DIM:],
                        preferred_element_type=F32,
                    )
                    for i in range(per)
                ],
                axis=0,
            )
            o = o1[slot, sel].reshape(flat) * keep + o16
            o = o + jnp.dot(p4.astype(BF16), v4, preferred_element_type=F32)
            if between is not None and group == NEAR // 2:
                between()
            mp[slot, sel] = (o / l).astype(BF16).reshape(per, rows, HEAD_DIM)
            m1[slot, sel] = (m_new * LN2 + jnp.log(l)).reshape(per, rows, HEAD_DIM)
        lane = iota((GRAN, HEAD_DIM), 1)
        for g in range(grans):
            cut = slice(g * FAR, (g + 1) * FAR)
            back = lambda a: lax.dot_general(
                a, shuffle, (((0,), (0,)), ((), ())), preferred_element_type=F32
            )
            merged = lax.dot_general(
                shuffle,
                mp[slot, :, cut].reshape(GRAN, HEAD_DIM),
                (((0,), (0,)), ((), ())),
                preferred_element_type=F32,
            )
            outs[hs, g * GRAN : (g + 1) * GRAN] = merged.astype(BF16)
            x = m1[slot, :, cut].reshape(GRAN, HEAD_DIM)
            high = x.astype(BF16).astype(F32)
            mid = (x - high).astype(BF16).astype(F32)
            low = x - high - mid
            terms = jnp.where(
                lane == 0, high, jnp.where(lane == 1, mid, jnp.where(lane == 2, low, 0.0))
            )
            lsend[hs, :, g * GRAN : (g + 1) * GRAN] = jnp.sum(
                back(terms.astype(BF16)), axis=0, keepdims=True
            )
        for cc in range(2):
            home = 2 * c + jb
            here = (home == y) & (cc == c)
            cut = slice(cc * length, (cc + 1) * length)

            @pl.when(here)
            def _(cut=cut):
                gath[t, y, h] = outs[hs, cut]
                logs[y, h] = lsend[hs, :, cut]

            start(o_copy(h, y, outs.at[hs, cut], 2 * hs + cc, at(z, home, cc)), jnp.logical_not(here))
            start(l_copy(h, y, lsend.at[hs, :, cut], 2 * hs + cc, at(z, home, cc)), jnp.logical_not(here))

    def o_copy(h, s, src, n, peer):
        return copy(src, gath.at[t, s, h], 28 + n, 28 + 2 * s + h, peer)

    def l_copy(h, s, src, n, peer):
        return copy(src, logs.at[s, h], 36 + n, 36 + 2 * s + h, peer)

    def piece(kind, h, k, owner, to):
        ref = gath.at[owner, seq(k), h]
        n = 44 + 8 * kind + 2 * k + h
        return copy(ref, ref, n, n, (sp, to))

    def collect(h, *ks):
        for k in ks:
            o_copy(h, seq(k), outs.at[0, :length], 0, (sp, right)).wait_recv()
        for a, b in zip(ks, reversed(ks)):
            start(piece(0, h, a, t, right))
            start(piece(1, h, b, t, left))

    def spread(h):
        piece(0, h, 0, t, right).start()
        piece(1, h, 0, t, left).start()

    def collect_mine(h):
        @pl.when(mine)
        def _():
            spread(h)

    def collect_twin(h):
        @pl.when(jnp.logical_not(mine))
        def _():
            o_copy(h, y, outs.at[0, :length], 0, (sp, right)).wait_recv()
            spread(h)

        sent.append((piece(0, h, 0, t, right), None))
        sent.append((piece(1, h, 0, t, left), None))

    def relay(h, k):
        if k in (0, 1):
            piece(0, h, k, left, right).wait_recv()
            start(piece(2, h, k, left, right))
        else:
            piece(1, h, k, right, left).wait_recv()
            start(piece(2, h, k, right, left))

    def rest(h, k):
        if k in (0, 1):
            piece(1, h, k, right, left).wait_recv()
        else:
            piece(0, h, k, left, right).wait_recv()
        piece(2, h, k, opposite, right).wait_recv()

    def share(h, k):
        term, square = None, None
        s = seq(k)
        x = jnp.concatenate([gath[n, s, h] for n in range(4)], axis=1).astype(F32)
        at_ = [slice(n * cols + h * HEAD_DIM, n * cols + (h + 1) * HEAD_DIM) for n in range(4)]
        g = jnp.concatenate([gain[:, a] for a in at_], axis=1)
        w = jnp.concatenate([wo[a] for a in at_], axis=0)
        term = jnp.dot((x * g).astype(BF16), w, preferred_element_type=F32)
        return term, jnp.sum(x * x, axis=1, keepdims=True)

    def partial(h, k):
        rest(h, k)
        acc[k], sq[k] = share(h, k)

    def finish(h, k):
        rest(h, k)
        term, square = share(h, k)
        square = square + sq[k]
        out[seq(k)] = (
            (acc[k] + term) * lax.rsqrt(square / wo.shape[0] + NORM_FLOOR)
        ).astype(BF16)

    forward(0, True)
    for ks in pairs:
        for k in ks:
            kv_send(1, k)
    gather_own(0)
    queries(0, 0)
    close_inner(0, 0)
    halo(0)
    gather_ends(0)
    close_outer(0, 0)
    attend_far(0, 0)
    collect_mine(0)
    for k in pairs[0]:
        q_send(1, k)
    forward(1, False)
    queries(0, 1)
    close_inner(0, 1)
    close_outer(0, 1)

    def half_way():
        collect_twin(0)
        forward(1, True)

    attend_far(0, 1, half_way)
    for k in pairs[1]:
        q_send(1, k)
    gather_own(1)
    collect(0, 2)
    relay(0, 0)
    queries(1, 0)
    close_inner(1, 0)
    halo(1)
    gather_ends(1)
    close_outer(1, 0)
    collect(0, 1, 3)
    attend_far(1, 0)
    relay(0, 2)
    collect_mine(1)
    queries(1, 1)
    close_inner(1, 1)
    close_outer(1, 1)
    collect_twin(1)
    attend_far(1, 1, lambda: relay(0, 1))
    collect(1, 2)
    relay(0, 3)
    relay(1, 0)
    got_wo.wait()
    partial(0, 0)
    partial(0, 2)
    done = len(sent)
    collect(1, 1, 3)
    relay(1, 2)
    partial(0, 1)
    partial(0, 3)

    def settle(some):
        for c_, there in some:
            if there is None:
                c_.wait_send()
            else:

                @pl.when(there)
                def _(c_=c_):
                    c_.wait_send()

    settle(sent[:done])
    for k in range(seqs):
        for h in range(heads):
            w = l_copy(h, seq(k), lsend.at[0, :, :length], 0, (sp, right))
            if k == 0:
                unless(mine, w)
            else:
                w.wait_recv()
    for s in range(seqs):
        for h in range(heads):
            log_out[s, h : h + 1] = logs[s, h]
    relay(1, 1)
    relay(1, 3)
    for k in (0, 2, 1, 3):
        finish(1, k)
    settle(sent[done:])


def layer(nsp, ntp, tokens, wq, wk, wv, wo, tables, gain):
    seqs, length, width = tokens.shape
    cols = wq.shape[1]
    heads = cols // HEAD_DIM
    block = 2 * length
    wide = REACH * FAR
    own = seqs // 2 * block
    span = own + 2 * wide
    window = block + 2 * wide
    rows = block // FAR
    near_rows = rows + 2 * FAR
    per = FAR // NEAR
    grans = block // GRAN
    hbm = pl.BlockSpec(memory_space=pl.ANY)
    vmem = pl.BlockSpec(memory_space=pltpu.VMEM)
    v = pltpu.VMEM
    return pl.pallas_call(
        functools.partial(layer_kernel, nsp),
        in_specs=[hbm] * 7 + [vmem] * 3,
        out_specs=[vmem, vmem],
        out_shape=[
            v((seqs, length, wo.shape[1]), BF16),
            v((seqs, heads, length), F32),
        ],
        scratch_shapes=[
            v(tokens.shape, BF16), v(wq.shape, BF16), v((heads, width, 2 * HEAD_DIM), BF16),
            v(wo.shape, BF16), v((length, HEAD_DIM), F32), v((length, HEAD_DIM), F32),
            v((heads, span, 2 * HEAD_DIM), BF16),
            v((heads, own, HEAD_DIM), BF16),
            v((seqs * heads, length, 2 * HEAD_DIM), BF16),
            v((seqs * heads, length, HEAD_DIM), BF16),
            v((ntp, seqs, heads, length, HEAD_DIM), BF16),
            v((2 * heads, block, HEAD_DIM), BF16),
            v((seqs, heads, 1, length), F32),
            v((2 * heads, 1, block), F32),
            v((heads, FAR, span // FAR, 2 * HEAD_DIM), BF16),
            v((2, FAR, rows, HEAD_DIM), BF16),
            v((2, FAR, rows, HEAD_DIM), BF16),
            v((GRAN, GRAN), BF16),
            v((2, grans, GRAN, GRAN + 2 * REACH), F32),
            v((2, per * rows, per * near_rows), F32),
            v((2, rows, window // FAR), F32),
            v((2, FAR, rows, HEAD_DIM), F32),
            v((2, FAR, rows, HEAD_DIM), F32),
            v((2, FAR, rows, HEAD_DIM), F32),
            v((seqs, length, wo.shape[1]), F32),
            v((seqs, length, 1), F32),
            pltpu.SemaphoreType.DMA((seqs + 8,)),
            pltpu.SemaphoreType.DMA((100,)),
            pltpu.SemaphoreType.DMA((100,)),
        ],
        compiler_params=pltpu.CompilerParams(
            collective_id=0, has_side_effects=True, vmem_limit_bytes=56 * 2**20
        ),
        name="layer",
    )(tokens, wq, wk, wv, wo, *tables, gain)


def store_kernel(mixed, logs, mixed_out, log_out, sem):
    copies = [
        pltpu.make_async_copy(mixed.at[s], mixed_out.at[s], sem.at[s])
        for s in range(mixed.shape[0])
    ]
    copies.append(pltpu.make_async_copy(logs, log_out, sem.at[mixed.shape[0]]))
    for c in copies:
        c.start()
    for c in copies:
        c.wait()


def store(mixed, logs):
    hbm = pl.BlockSpec(memory_space=pl.ANY)
    vmem = pl.BlockSpec(memory_space=pltpu.VMEM)
    return pl.pallas_call(
        store_kernel,
        in_specs=[vmem] * 2,
        out_specs=[hbm] * 2,
        out_shape=[jax.ShapeDtypeStruct(a.shape, a.dtype) for a in (mixed, logs)],
        scratch_shapes=[pltpu.SemaphoreType.DMA((mixed.shape[0] + 1,))],
        compiler_params=pltpu.CompilerParams(vmem_limit_bytes=2**20),
        name="store",
    )(mixed, logs)


def shards(tokens, query_weight, key_weight, value_weight, out_gain, out_weight):
    length = tokens.shape[1]
    nsp = lax.axis_size("sp")
    frequency = ROPE_BASE ** (-np.arange(HEAD_DIM // 2) / (HEAD_DIM // 2))
    frequency = np.tile(frequency, 2)[None, :]
    step = np.arange(length)[:, None] * frequency
    base = (np.arange(nsp) * length)[:, None] * frequency
    tables = [
        jnp.asarray(f(a).astype(np.float32)) for a in (step, base) for f in (np.cos, np.sin)
    ]
    return tuple(
        store(*layer(
            nsp, lax.axis_size("tp"), tokens, query_weight, key_weight, value_weight,
            out_weight, tables, out_gain[None, :],
        ))
    )


def solution(mesh):
    return jax.shard_map(
        shards,
        mesh=mesh,
        in_specs=(
            P(None, "sp", None),
            P(None, "tp"),
            P(None, "tp"),
            P(None, "tp"),
            P(),
            P(None, "tp"),
        ),
        out_specs=(P(None, "sp", "tp"), P(None, "tp", "sp")),
        check_vma=False,
    )
```

```python
import functools
import math

import jax
import jax.numpy as jnp
import numpy as np
from jax import lax
from jax.experimental import pallas as pl
from jax.experimental.pallas import tpu as pltpu
from jax.sharding import PartitionSpec as P

HEAD_DIM = 128
REACH = 64
FAR = 16
NEAR = 4
GRAN = FAR * FAR
ROPE_BASE = 10000.0
MASK_FILL = -1e30
NORM_FLOOR = 1e-06
LOG2E = 1.0 / math.log(2.0)
LN2 = math.log(2.0)
F32 = jnp.float32
BF16 = jnp.bfloat16

MESH = pl.DeviceIdType.MESH


def iota(shape, dim):
    return lax.broadcasted_iota(jnp.int32, shape, dim)


def perm_token(p):
    slot = p // FAR
    a = p % FAR
    residue = slot // NEAR + NEAR * (slot % (FAR // NEAR))
    return a * FAR + residue


def dot_t(a, b):
    return lax.dot_general(a, b, (((1,), (1,)), ((), ())), preferred_element_type=F32)


def layer_kernel(
    nsp, tok_h, wq_h, wk_h, wv_h, wo_h, cos_h, sin_h, cos_base, sin_base, gain,
    out, log_out,
    tok, wq, wkv, wo, cos, sin, kn, qn, kvs, qs, gath, outs, logs, lsend,
    kp, qp, mp, perm, bias1, bias4, bias16, o1, m1, l1, acc, sq,
    load_sem, send_sem, recv_sem,
):
    seqs, length = tok.shape[:2]
    block = 2 * length
    grans = block // GRAN
    wide = REACH * FAR
    side = wide // GRAN
    own = seqs // 2 * block
    span = own + 2 * wide
    window = block + 2 * wide
    rows = block // FAR
    key_rows = window // FAR
    near_rows = rows + 2 * FAR
    cols = wq.shape[1]
    heads = cols // HEAD_DIM
    ends = wide // GRAN
    stop = ends + own // GRAN
    total = nsp * length
    scale = HEAD_DIM**-0.5 * LOG2E
    sp, t = lax.axis_index("sp"), lax.axis_index("tp")
    plane = 2 * seqs
    z, y, c = sp // plane, (sp // 2) % seqs, sp % 2
    worker = y // 2
    mine = worker == c
    place = 2 * (y % 2) + c
    right, left, opposite = (t + 1) % 4, (t + 3) % 4, (t + 2) % 4
    part = 2 * z + c
    last = 2 * (nsp // plane) - 1
    above, below = part < last, part > 0

    def at(zz, yy, cc):
        return (zz * plane + yy * 2 + cc, t)

    def half_at(p):
        return at(p // 2, y, p % 2)

    def seq(k):
        return (y + k) % seqs

    loads = []

    def load(src, dst):
        copy = pltpu.make_async_copy(src, dst, load_sem.at[len(loads)])
        copy.start()
        loads.append(copy)
        return copy

    def lanes(n):
        return slice(n * HEAD_DIM, (n + 1) * HEAD_DIM)

    def load_kv(h):
        return (
            load(wk_h.at[:, lanes(h)], wkv.at[h, :, lanes(0)]),
            load(wv_h.at[:, lanes(h)], wkv.at[h, :, lanes(1)]),
        )

    def load_tok(k):
        return load(tok_h.at[seq(k)], tok.at[k])

    pairs = ((2, 0), (1, 3))
    got_rope = (load(cos_h, cos), load(sin_h, sin))
    got_first = (*load_kv(0), load_tok(2))
    got_second = [load_tok(k) for k in pairs[1]]
    got_wq = (load(wq_h, wq), load_tok(0))
    got_third = load_kv(1)
    got_wo = load(wo_h, wo)

    barrier = pltpu.get_barrier_semaphore()

    def greet(peer):
        pl.semaphore_signal(barrier, inc=1, device_id=peer, device_id_type=MESH)

    for k in range(1, seqs):
        greet(at(z, seq(k), worker))
    for i in range(2):
        for cc in range(2):

            @pl.when(jnp.logical_not((2 * c + i == y) & (cc == c)))
            def _(i=i, cc=cc):
                greet(at(z, 2 * c + i, cc))

    @pl.when(jnp.logical_not(mine))
    def _():
        greet(at(z, y, worker))

    greet((sp, right))
    greet((sp, left))

    @pl.when(above)
    def _():
        greet(half_at(part + 1))

    @pl.when(below)
    def _():
        greet(half_at(part - 1))

    count = (
        2 * seqs + 2 - 2 * mine.astype(jnp.int32)
        + above.astype(jnp.int32) + below.astype(jnp.int32)
    )

    @pl.when(jnp.logical_not(below))
    def _():
        for h in range(heads):
            kn[h, 0:wide] = jnp.zeros((wide, kn.shape[2]), BF16)

    @pl.when(jnp.logical_not(above))
    def _():
        for h in range(heads):
            kn[h, wide + own : span] = jnp.zeros((wide, kn.shape[2]), BF16)

    def copy(src, dst, send, recv, peer):
        return pltpu.make_async_remote_copy(
            src_ref=src, dst_ref=dst, send_sem=send_sem.at[send], recv_sem=recv_sem.at[recv],
            device_id=peer, device_id_type=MESH,
        )

    sent = []

    def start(c, there=None):
        if there is None:
            c.start()
        else:

            @pl.when(there)
            def _():
                c.start()

        sent.append((c, there))

    def unless(cond, c):
        @pl.when(jnp.logical_not(cond))
        def _():
            c.wait_recv()

    def chunk(j):
        return pl.ds(pl.multiple_of(wide + j * length, HEAD_DIM), length)

    def q_chunk(j):
        return pl.ds(pl.multiple_of(j * length, HEAD_DIM), length)

    piece_rows = length // 2

    def kv_copy(h, k, j, i):
        at_ = pl.ds(pl.multiple_of(wide + j * length + i * piece_rows, REACH), piece_rows)
        n = 68 * i + h * 4
        return copy(
            kvs.at[k * heads + h, pl.ds(i * piece_rows, piece_rows)], kn.at[h, at_], n + k, n + j,
            at(z, seq(k), worker),
        )

    def q_copy(h, k, j):
        return copy(
            qs.at[k * heads + h], qn.at[h, q_chunk(j)], 8 + h * 4 + k, 8 + h * 4 + j,
            at(z, seq(k), worker),
        )

    def is_here(j):
        return (2 * c + j // 2 == y) & (j % 2 == c)

    def kv_send(h, k):
        if k == 0:

            @pl.when(mine)
            def _():
                kn[h, chunk(place)] = kvs[h]

        for i in range(2):
            start(kv_copy(h, k, place, i), jnp.logical_not(mine) if k == 0 else None)

    def q_send(h, k):
        if k == 0:

            @pl.when(mine)
            def _():
                qn[h, q_chunk(place)] = qs[h]

        start(q_copy(h, k, place), jnp.logical_not(mine) if k == 0 else None)

    spans = [(max(n * piece_rows, own - wide), (n + 1) * piece_rows) for n in range(8)]
    cuts_up = [(wide + a, b - a) for a, b in spans if b > a]
    spans = [(n * piece_rows, min((n + 1) * piece_rows, wide)) for n in range(8)]
    cuts_down = [(wide + a, b - a) for a, b in spans if b > a]

    def up(h, p):
        row, size = cuts_up[p]
        return copy(
            kn.at[h, row : row + size], kn.at[h, row - own : row - own + size],
            76 + 6 * h + p, 76 + 6 * h + p, half_at(part + 1),
        )

    def down(h, p):
        row, size = cuts_down[p]
        return copy(
            kn.at[h, row : row + size], kn.at[h, row + own : row + own + size],
            88 + 6 * h + p, 88 + 6 * h + p, half_at(part - 1),
        )

    flip = y % 2 == 1

    def forward(h, far):
        def relay_in(js):
            for n in [2 * j + i for j in js for i in range(2)]:
                unless(is_here(n // 2), kv_copy(h, 0, n // 2, n % 2))
                if n < 6:

                    @pl.when(below)
                    def _(n=n):
                        down(h, n).start()

                if n > 1:

                    @pl.when(above)
                    def _(n=n):
                        up(h, n - 2).start()

        @pl.when(flip != far)
        def _():
            relay_in((2, 3))

        @pl.when(flip == far)
        def _():
            relay_in((0, 1))

        if far:
            for p in range(6):
                sent.append((down(h, p), below))
                sent.append((up(h, p), above))

    def halo(h):
        for p in range(6):
            unless(jnp.logical_not(below), up(h, p))
            unless(jnp.logical_not(above), down(h, p))

    def turned(one, by=None):
        a = one * cos[...] + pltpu.roll(one, HEAD_DIM // 2, 1) * sin[...]
        return (a if by is None else a * by).astype(BF16)

    def store_kv(h, k, a):
        kvs[k * heads + h, :, lanes(0)] = turned(a[:, lanes(0)])
        kvs[k * heads + h, :, lanes(1)] = a[:, lanes(1)].astype(BF16)

    def project_kv(h, ks):
        both = [jnp.dot(tok[k], wkv[h], preferred_element_type=F32) for k in ks]
        for k, a in zip(ks, both):
            store_kv(h, k, a)

    def project_q(ks):
        both = [jnp.dot(tok[k], wq[...], preferred_element_type=F32) for k in ks]
        for k, a in zip(ks, both):
            for h in range(heads):
                qs[k * heads + h] = turned(a[:, lanes(h)], scale)

    cos_at, sin_at = cos_base[pl.ds(sp, 1)], sin_base[pl.ds(sp, 1)]
    sign = jnp.where(iota(cos.shape, 1) < HEAD_DIM // 2, -1.0, 1.0)
    for c_ in got_rope:
        c_.wait()
    cos_step, sin_step = cos[...], sin[...]
    cos[...] = cos_step * cos_at - sin_step * sin_at
    sin[...] = (sin_step * cos_at + cos_step * sin_at) * sign
    for c_ in got_first:
        c_.wait()
    cut = length // 2
    halves = [
        jnp.dot(tok[2, i * cut : (i + 1) * cut], wkv[0], preferred_element_type=F32)
        for i in range(2)
    ]
    store_kv(0, 2, jnp.concatenate(halves, axis=0))
    pl.semaphore_wait(barrier, count)
    kv_send(0, 2)
    for c_ in got_second:
        c_.wait()
    project_kv(0, pairs[1])
    for k in pairs[1]:
        kv_send(0, k)
    for c_ in got_wq:
        c_.wait()
    halves = [
        jnp.dot(tok[0, i * cut : (i + 1) * cut], wkv[0], preferred_element_type=F32)
        for i in range(2)
    ]
    store_kv(0, 0, jnp.concatenate(halves, axis=0))
    kv_send(0, 0)
    for ks in pairs:
        project_q(ks)
        for k in ks:
            q_send(0, k)
    for c_ in got_third:
        c_.wait()
    for ks in pairs:
        project_kv(1, ks)

    forward(0, False)
    perm[...] = jnp.where(
        iota((GRAN, GRAN), 1) == perm_token(iota((GRAN, GRAN), 0)), 1.0, 0.0
    ).astype(BF16)
    per = FAR // NEAR
    for jb in range(2):
        origin = part * own - wide + jb * block
        shape = (GRAN, GRAN + 2 * REACH)
        token = perm_token(iota(shape, 0))
        for g in range(grans):
            q_at = wide + g * GRAN + token
            k_at = wide + g * GRAN - REACH + iota(shape, 1)
            ok = (jnp.abs(k_at - q_at) <= REACH) & (k_at + origin >= 0) & (k_at + origin < total)
            bias1[jb, g] = jnp.where(ok, 0.0, MASK_FILL)
        shape = (per * rows, per * near_rows)
        row, col = iota(shape, 0), iota(shape, 1)
        q_at = (row % rows + side * FAR) * FAR + NEAR * (row // rows)
        k_at = (col % near_rows + (side - 1) * FAR) * FAR + NEAR * (col // near_rows)
        ok = (jnp.abs(k_at - q_at) <= REACH * NEAR) & (k_at + origin >= 0) & (k_at + origin < total)
        bias4[jb] = jnp.where(ok, 0.0, MASK_FILL)
        shape = (rows, key_rows)
        q_at = iota(shape, 0) + side * FAR
        k_at = iota(shape, 1)
        ok = (
            (jnp.abs(k_at - q_at) <= REACH)
            & (k_at * FAR + origin >= 0)
            & (k_at * FAR + origin < total)
        )
        bias16[jb] = jnp.where(ok, 0.0, MASK_FILL)

    def gather_keys(h, chunks):
        for j in chunks:
            moved = jnp.dot(
                perm[...], kn[h, j * GRAN : (j + 1) * GRAN], preferred_element_type=F32
            )
            moved = moved.astype(BF16).reshape(FAR, FAR, 2 * HEAD_DIM)
            kp[h, :, j * FAR : (j + 1) * FAR] = moved

    def gather_own(h):
        gather_keys(h, range(ends, stop))

    def gather_ends(h):
        gather_keys(h, [*range(ends), *range(stop, span // GRAN)])

    def queries(h, step):
        for i in range(2):
            j = (step + y) % 2 * 2 + i
            unless(is_here(j), q_copy(h, 0, j))

    def close(h, step, g):
        jb = (step + y) % 2
        q_at = pl.multiple_of(jb * block + g * GRAN, GRAN)
        near = pl.ds(pl.multiple_of(q_at + wide - REACH, REACH), GRAN + 2 * REACH)
        sl = pl.ds(pl.multiple_of(g * FAR, FAR), FAR)
        moved = jnp.dot(perm[...], qn[h, pl.ds(q_at, GRAN)], preferred_element_type=F32)
        moved = moved.astype(BF16)
        qp[step, :, sl] = moved.reshape(FAR, FAR, HEAD_DIM)
        k = kn[h, near, lanes(0)]
        v = kn[h, near, lanes(1)]
        sc = dot_t(moved, k) + bias1[jb, g]
        m = jnp.max(sc, axis=1, keepdims=True)
        p = jnp.exp2(sc - m)
        l = jnp.sum(p, axis=1, keepdims=True)
        o = jnp.dot(p.astype(BF16), v, preferred_element_type=F32)
        cut = (FAR, FAR, HEAD_DIM)
        o1[step, :, sl] = o.reshape(cut)
        m1[step, :, sl] = jnp.broadcast_to(m, o.shape).reshape(cut)
        l1[step, :, sl] = jnp.broadcast_to(l, o.shape).reshape(cut)

    def close_inner(h, step):
        for i in range(1, grans):
            close(h, step, i - (step + y) % 2)

    def close_outer(h, step):
        close(h, step, (step + y) % 2 * (grans - 1))

    def attend_far(h, step, between=None):
        slot = step
        hs = 2 * h + step
        jb = (step + y) % 2
        shuffle = perm[...]
        near = pl.ds(pl.multiple_of((side - 1) * FAR + jb * rows, FAR), near_rows)
        whole = pl.ds(pl.multiple_of(jb * rows, FAR), key_rows)
        for group in range(NEAR):
            sel = slice(group * per, (group + 1) * per)
            flat = (per * rows, HEAD_DIM)
            q = qp[slot, sel].reshape(flat)
            k4 = kp[h, sel, near, :HEAD_DIM].reshape(-1, HEAD_DIM)
            v4 = kp[h, sel, near, HEAD_DIM:].reshape(-1, HEAD_DIM)
            s4 = dot_t(q, k4) + bias4[jb]
            b16 = bias16[jb]
            s16 = jnp.concatenate(
                [
                    dot_t(qp[slot, group * per + i], kp[h, group * per + i, whole, :HEAD_DIM]) + b16
                    for i in range(per)
                ],
                axis=0,
            )
            m_old = m1[slot, sel].reshape(flat)
            m_row = jnp.maximum(
                jnp.max(s4, axis=1, keepdims=True), jnp.max(s16, axis=1, keepdims=True)
            )
            m_new = jnp.maximum(m_old, m_row)
            m_col = m_new[:, :1]
            keep = jnp.exp2(m_old - m_new)
            p4 = jnp.exp2(s4 - m_col)
            p16 = jnp.exp2(s16 - m_col)
            l = l1[slot, sel].reshape(flat) * keep + (
                jnp.sum(p4, axis=1, keepdims=True) + jnp.sum(p16, axis=1, keepdims=True)
            )
            p16 = p16.astype(BF16)
            o16 = jnp.concatenate(
                [
                    jnp.dot(
                        p16[i * rows : (i + 1) * rows],
                        kp[h, group * per + i, whole, HEAD_DIM:],
                        preferred_element_type=F32,
                    )
                    for i in range(per)
                ],
                axis=0,
            )
            o = o1[slot, sel].reshape(flat) * keep + o16
            o = o + jnp.dot(p4.astype(BF16), v4, preferred_element_type=F32)
            if between is not None and group == NEAR // 2:
                between()
            mp[slot, sel] = (o / l).astype(BF16).reshape(per, rows, HEAD_DIM)
            m1[slot, sel] = (m_new * LN2 + jnp.log(l)).reshape(per, rows, HEAD_DIM)
        lane = iota((GRAN, HEAD_DIM), 1)
        for g in range(grans):
            cut = slice(g * FAR, (g + 1) * FAR)
            back = lambda a: lax.dot_general(
                a, shuffle, (((0,), (0,)), ((), ())), preferred_element_type=F32
            )
            merged = lax.dot_general(
                shuffle,
                mp[slot, :, cut].reshape(GRAN, HEAD_DIM),
                (((0,), (0,)), ((), ())),
                preferred_element_type=F32,
            )
            outs[hs, g * GRAN : (g + 1) * GRAN] = merged.astype(BF16)
            x = m1[slot, :, cut].reshape(GRAN, HEAD_DIM)
            high = x.astype(BF16).astype(F32)
            mid = (x - high).astype(BF16).astype(F32)
            low = x - high - mid
            terms = jnp.where(
                lane == 0, high, jnp.where(lane == 1, mid, jnp.where(lane == 2, low, 0.0))
            )
            lsend[hs, :, g * GRAN : (g + 1) * GRAN] = jnp.sum(
                back(terms.astype(BF16)), axis=0, keepdims=True
            )
        for cc in range(2):
            home = 2 * c + jb
            here = (home == y) & (cc == c)
            cut = slice(cc * length, (cc + 1) * length)

            @pl.when(here)
            def _(cut=cut):
                gath[t, y, h] = outs[hs, cut]
                logs[y, h] = lsend[hs, :, cut]

            start(o_copy(h, y, outs.at[hs, cut], 2 * hs + cc, at(z, home, cc)), jnp.logical_not(here))
            start(l_copy(h, y, lsend.at[hs, :, cut], 2 * hs + cc, at(z, home, cc)), jnp.logical_not(here))

    def o_copy(h, s, src, n, peer):
        return copy(src, gath.at[t, s, h], 28 + n, 28 + 2 * s + h, peer)

    def l_copy(h, s, src, n, peer):
        return copy(src, logs.at[s, h], 36 + n, 36 + 2 * s + h, peer)

    def piece(kind, h, k, owner, to):
        ref = gath.at[owner, seq(k), h]
        n = 44 + 8 * kind + 2 * k + h
        return copy(ref, ref, n, n, (sp, to))

    def collect(h, *ks):
        for k in ks:
            o_copy(h, seq(k), outs.at[0, :length], 0, (sp, right)).wait_recv()
        for a, b in zip(ks, reversed(ks)):
            start(piece(0, h, a, t, right))
            start(piece(1, h, b, t, left))

    def spread(h):
        piece(0, h, 0, t, right).start()
        piece(1, h, 0, t, left).start()

    def collect_mine(h):
        @pl.when(mine)
        def _():
            spread(h)

    def collect_twin(h):
        @pl.when(jnp.logical_not(mine))
        def _():
            o_copy(h, y, outs.at[0, :length], 0, (sp, right)).wait_recv()
            spread(h)

        sent.append((piece(0, h, 0, t, right), None))
        sent.append((piece(1, h, 0, t, left), None))

    def relay(h, k):
        if k in (0, 1):
            piece(0, h, k, left, right).wait_recv()
            start(piece(2, h, k, left, right))
        else:
            piece(1, h, k, right, left).wait_recv()
            start(piece(2, h, k, right, left))

    def rest(h, k):
        if k in (0, 1):
            piece(1, h, k, right, left).wait_recv()
        else:
            piece(0, h, k, left, right).wait_recv()
        piece(2, h, k, opposite, right).wait_recv()

    def share(h, k):
        term, square = None, None
        s = seq(k)
        x = jnp.concatenate([gath[n, s, h] for n in range(4)], axis=1).astype(F32)
        at_ = [slice(n * cols + h * HEAD_DIM, n * cols + (h + 1) * HEAD_DIM) for n in range(4)]
        g = jnp.concatenate([gain[:, a] for a in at_], axis=1)
        w = jnp.concatenate([wo[a] for a in at_], axis=0)
        term = jnp.dot((x * g).astype(BF16), w, preferred_element_type=F32)
        return term, jnp.sum(x * x, axis=1, keepdims=True)

    def partial(h, k):
        rest(h, k)
        acc[k], sq[k] = share(h, k)

    def finish(h, k):
        rest(h, k)
        term, square = share(h, k)
        square = square + sq[k]
        out[seq(k)] = (
            (acc[k] + term) * lax.rsqrt(square / wo.shape[0] + NORM_FLOOR)
        ).astype(BF16)

    forward(0, True)
    for ks in pairs:
        for k in ks:
            kv_send(1, k)
    gather_own(0)
    queries(0, 0)
    close_inner(0, 0)
    halo(0)
    gather_ends(0)
    close_outer(0, 0)
    attend_far(0, 0)
    collect_mine(0)
    for k in pairs[0]:
        q_send(1, k)
    forward(1, False)
    queries(0, 1)
    close_inner(0, 1)
    close_outer(0, 1)

    def half_way():
        collect_twin(0)
        forward(1, True)

    attend_far(0, 1, half_way)
    for k in pairs[1]:
        q_send(1, k)
    gather_own(1)
    collect(0, 2)
    relay(0, 0)
    queries(1, 0)
    close_inner(1, 0)
    halo(1)
    gather_ends(1)
    close_outer(1, 0)
    collect(0, 1)
    collect(0, 3)
    attend_far(1, 0)
    relay(0, 2)
    collect_mine(1)
    queries(1, 1)
    close_inner(1, 1)
    close_outer(1, 1)
    collect_twin(1)
    attend_far(1, 1, lambda: relay(0, 1))
    collect(1, 2)
    relay(0, 3)
    relay(1, 0)
    got_wo.wait()
    partial(0, 0)
    partial(0, 2)
    done = len(sent)
    collect(1, 1, 3)
    relay(1, 2)
    partial(0, 1)
    partial(0, 3)

    def settle(some):
        for c_, there in some:
            if there is None:
                c_.wait_send()
            else:

                @pl.when(there)
                def _(c_=c_):
                    c_.wait_send()

    settle(sent[:done])
    for k in range(seqs):
        for h in range(heads):
            w = l_copy(h, seq(k), lsend.at[0, :, :length], 0, (sp, right))
            if k == 0:
                unless(mine, w)
            else:
                w.wait_recv()
    for s in range(seqs):
        for h in range(heads):
            log_out[s, h : h + 1] = logs[s, h]
    relay(1, 1)
    relay(1, 3)
    for k in (0, 2, 1, 3):
        finish(1, k)
    settle(sent[done:])


def layer(nsp, ntp, tokens, wq, wk, wv, wo, tables, gain):
    seqs, length, width = tokens.shape
    cols = wq.shape[1]
    heads = cols // HEAD_DIM
    block = 2 * length
    wide = REACH * FAR
    own = seqs // 2 * block
    span = own + 2 * wide
    window = block + 2 * wide
    rows = block // FAR
    near_rows = rows + 2 * FAR
    per = FAR // NEAR
    grans = block // GRAN
    hbm = pl.BlockSpec(memory_space=pl.ANY)
    vmem = pl.BlockSpec(memory_space=pltpu.VMEM)
    v = pltpu.VMEM
    return pl.pallas_call(
        functools.partial(layer_kernel, nsp),
        in_specs=[hbm] * 7 + [vmem] * 3,
        out_specs=[vmem, vmem],
        out_shape=[
            v((seqs, length, wo.shape[1]), BF16),
            v((seqs, heads, length), F32),
        ],
        scratch_shapes=[
            v(tokens.shape, BF16), v(wq.shape, BF16), v((heads, width, 2 * HEAD_DIM), BF16),
            v(wo.shape, BF16), v((length, HEAD_DIM), F32), v((length, HEAD_DIM), F32),
            v((heads, span, 2 * HEAD_DIM), BF16),
            v((heads, own, HEAD_DIM), BF16),
            v((seqs * heads, length, 2 * HEAD_DIM), BF16),
            v((seqs * heads, length, HEAD_DIM), BF16),
            v((ntp, seqs, heads, length, HEAD_DIM), BF16),
            v((2 * heads, block, HEAD_DIM), BF16),
            v((seqs, heads, 1, length), F32),
            v((2 * heads, 1, block), F32),
            v((heads, FAR, span // FAR, 2 * HEAD_DIM), BF16),
            v((2, FAR, rows, HEAD_DIM), BF16),
            v((2, FAR, rows, HEAD_DIM), BF16),
            v((GRAN, GRAN), BF16),
            v((2, grans, GRAN, GRAN + 2 * REACH), F32),
            v((2, per * rows, per * near_rows), F32),
            v((2, rows, window // FAR), F32),
            v((2, FAR, rows, HEAD_DIM), F32),
            v((2, FAR, rows, HEAD_DIM), F32),
            v((2, FAR, rows, HEAD_DIM), F32),
            v((seqs, length, wo.shape[1]), F32),
            v((seqs, length, 1), F32),
            pltpu.SemaphoreType.DMA((seqs + 8,)),
            pltpu.SemaphoreType.DMA((100,)),
            pltpu.SemaphoreType.DMA((100,)),
        ],
        compiler_params=pltpu.CompilerParams(
            collective_id=0, has_side_effects=True, vmem_limit_bytes=56 * 2**20
        ),
        name="layer",
    )(tokens, wq, wk, wv, wo, *tables, gain)


def store_kernel(mixed, logs, mixed_out, log_out, sem):
    copies = [
        pltpu.make_async_copy(mixed.at[s], mixed_out.at[s], sem.at[s])
        for s in range(mixed.shape[0])
    ]
    copies.append(pltpu.make_async_copy(logs, log_out, sem.at[mixed.shape[0]]))
    for c in copies:
        c.start()
    for c in copies:
        c.wait()


def store(mixed, logs):
    hbm = pl.BlockSpec(memory_space=pl.ANY)
    vmem = pl.BlockSpec(memory_space=pltpu.VMEM)
    return pl.pallas_call(
        store_kernel,
        in_specs=[vmem] * 2,
        out_specs=[hbm] * 2,
        out_shape=[jax.ShapeDtypeStruct(a.shape, a.dtype) for a in (mixed, logs)],
        scratch_shapes=[pltpu.SemaphoreType.DMA((mixed.shape[0] + 1,))],
        compiler_params=pltpu.CompilerParams(vmem_limit_bytes=2**20),
        name="store",
    )(mixed, logs)


def shards(tokens, query_weight, key_weight, value_weight, out_gain, out_weight):
    length = tokens.shape[1]
    nsp = lax.axis_size("sp")
    frequency = ROPE_BASE ** (-np.arange(HEAD_DIM // 2) / (HEAD_DIM // 2))
    frequency = np.tile(frequency, 2)[None, :]
    step = np.arange(length)[:, None] * frequency
    base = (np.arange(nsp) * length)[:, None] * frequency
    tables = [
        jnp.asarray(f(a).astype(np.float32)) for a in (step, base) for f in (np.cos, np.sin)
    ]
    return tuple(
        store(*layer(
            nsp, lax.axis_size("tp"), tokens, query_weight, key_weight, value_weight,
            out_weight, tables, out_gain[None, :],
        ))
    )


def solution(mesh):
    return jax.shard_map(
        shards,
        mesh=mesh,
        in_specs=(
            P(None, "sp", None),
            P(None, "tp"),
            P(None, "tp"),
            P(None, "tp"),
            P(),
            P(None, "tp"),
        ),
        out_specs=(P(None, "sp", "tp"), P(None, "tp", "sp")),
        check_vma=False,
    )
```
